32 devices in a mesh: sp: 4 (over y, x), tp: 8 (over z, core).
Axes of the slice: x: 2, y: 2, z: 4, core: 2. Of those that a mesh axis runs over, the one named last changes fastest.
Arguments:
- lru_input: bfloat16 [1024, 2048], P('sp', 'tp'), may hold values from -27 to 27
- gate_input: bfloat16 [1024, 2048], P('sp', 'tp'), may hold values from -6 to 6
- documents: int32 [1024], P('sp'), may hold values from 0 to 1, never falling along the last dimension, each value on 1 to 768 neighbouring positions
- conv_taps: bfloat16 [4, 2048], P(None, 'tp'), may hold values from -3 to 3
- rate_weight: bfloat16 [16, 128, 128], P('tp'), may hold values from -0.5 to 0.5
- inlet_weight: bfloat16 [16, 128, 128], P('tp'), may hold values from -0.5 to 0.5
- decay_param: float32 [2048], P('tp')
- lru_gain: float32 [2048], P('tp'), may hold values from 0.1 to 1.9
- out_weight: bfloat16 [2048, 2048], P('tp'), may hold values from -0.125 to 0.125
- residual: bfloat16 [1024, 2048], P('sp'), may hold values from -6 to 6
- ffn_gain: float32 [2048], replicated, may hold values from 0.1 to 1.9
- routes: int32 [1024, 2], P('sp'), may hold values from 0 to 3, all different within a row; in each aligned block of 32 rows (0 to 31, 32 to 63, ...) at most 32 rows name the same one
- route_weights: float32 [1024, 2], P('sp'), may hold values from 0.1 to 0.9
- w_gate: bfloat16 [4, 2048, 6144], P('sp', None, 'tp'), may hold values from -0.125 to 0.125
- w_up: bfloat16 [4, 2048, 6144], P('sp', None, 'tp'), may hold values from -0.125 to 0.125
- w_down: bfloat16 [4, 6144, 2048], P('sp', 'tp'), may hold values from -0.078125 to 0.078125
Outputs:
- mixed_out: bfloat16 [1024, 2048], P(('sp', 'tp'))
The draws below stay inside these ranges and needn't reach their ends.
Inputs may be any that keep to these rules, and one draw needn't show every extreme that they name: `documents`: document numbers start at 0 and never fall along the sequence; a document spans at most 768 positions. `routes`: each row names 2 different experts. In each aligned block of 32 rows no expert is named by more than 32 rows, a bound that some block reaches.
All inputs are finite; a program needn't handle non-finite values.
Results may differ from the reference program's by a relative error of at most 0.017.
Values may be sent and summed in bfloat16 or wider, within the bound.
A program may use at most 64 MiB of HBM per device.

```python
import math
import jax
import jax.numpy as jnp
import numpy as np
from jax import lax

D = 2048
D_RNN = 2048
LRU_BLOCKS = 16
LRU_BLOCK = 128
CONV_TAPS = 4
FF = 6144
TOP = 2
TOKENS = 1024
ROUTE_ROWS = 32
EXPERTS = 4
CAP = 32
DOCS = 2
DOC_MOST = 768
N_TP = 8


def draw_lru_input(key, part):
    base_key, group_key, span_key = jax.random.split(jax.random.fold_in(key, 11), 3)
    group_levels = jax.random.uniform(group_key, (LRU_BLOCKS,), jnp.float32, -1.2, 1.2)
    span_levels = jax.random.uniform(span_key, (TOKENS // 64,), jnp.float32, -0.7, 0.7)
    channel_scale = jnp.repeat(jnp.exp(group_levels), LRU_BLOCK)
    position_scale = jnp.repeat(jnp.exp(span_levels), 64)
    base_values = jnp.clip(jax.random.normal(base_key, (TOKENS, D_RNN), jnp.float32), -4.0, 4.0)
    return (base_values * channel_scale[None, :] * position_scale[:, None]).astype(jnp.bfloat16)


def draw_decay_param(key, part):
    pick_key, slow_key, fast_key = jax.random.split(jax.random.fold_in(key, 23), 3)
    slow_share = 0.5
    slow_pick = jax.random.uniform(pick_key, (D_RNN,), jnp.float32) < slow_share
    slow_value = math.log(2.5 * TOKENS) + jax.random.uniform(slow_key, (D_RNN,), jnp.float32, 0.0, 1.5)
    fast_value = jnp.log(jax.random.uniform(fast_key, (D_RNN,), jnp.float32, 120.0, 400.0))
    return jnp.where(slow_pick, slow_value, fast_value).astype(jnp.float32)


def block_levels(rng, extent, pieces, smallest, largest):
    level = 1.0
    for axis_at, parts in pieces:
        steps = jax.random.uniform(jax.random.fold_in(jax.random.fold_in(rng, 6), axis_at), (parts,), jnp.float32, smallest / len(pieces), largest / len(pieces))
        level = level * jnp.repeat(jnp.exp(steps), extent[axis_at] // parts).reshape((-1,) + (1,) * (len(extent) - 1 - axis_at))
    return level


def profile(number_of, total, reach, slope):
    weights = [(1 << 20) // math.isqrt(standing ** slope) + 1 for standing in range(2, number_of + 1)]
    surplus, counts = total - reach - (number_of - 1), [1] * (number_of - 1)
    while surplus > 0:
        movable = [i for i in range(number_of - 1) if counts[i] < reach]
        pool, budget = sum([weights[i] for i in movable]), surplus
        for i in movable:
            more = min(reach - counts[i], max(1, budget * weights[i] // pool), surplus)
            counts[i] = counts[i] + more
            surplus = surplus - more
    return np.array([reach] + counts)


def ragged_sizes(key, count, total, bound, lean):
    if count == 2:
        one = jax.random.randint(key, (), max(1, total - bound), min(bound, total - 1) + 1)
        return jnp.stack([one, total - one])
    lengths = jnp.asarray(profile(count, total, bound, lean), jnp.int32)
    twos = (count - 1) // 2
    donor, receiver = lengths[1:1 + 2 * twos:2], lengths[2:2 + 2 * twos:2]
    slack = jnp.minimum(donor - 1, bound - receiver)
    moved = jax.random.randint(jax.random.fold_in(key, 1), (twos,), 0, 1 << 20) % (slack + 1)
    lengths = lengths.at[1:1 + 2 * twos:2].set(donor - moved).at[2:2 + 2 * twos:2].set(receiver + moved)
    return lengths[jax.random.permutation(jax.random.fold_in(key, 2), count)]


def deal_out(key, own, number, rows, number_of, top, limit, lean):
    sequence = jax.random.permutation(key, number_of)
    packed, common = load_shares(number_of, rows * top, limit, lean, True), load_shares(number_of, rows * top, limit, lean, False)
    places = jnp.arange(number_of)

    def named(tallies, rotation):
        used = int((tallies > 0).sum())
        fixed = max(1, used // 4)
        passed = fixed + (places - fixed + rotation * (used - fixed)) % max(1, number_of - fixed)
        return jnp.zeros((number_of,), jnp.int32).at[sequence[jnp.where(places < fixed, places, passed)]].set(jnp.asarray(tallies, jnp.int32))

    tallies = jnp.where(number % 4 == 0, named(packed, number // 4), named(common, number - number // 4 - 1))
    mixed = jax.random.permutation(jax.random.fold_in(own, 3), number_of)
    donor, sink = mixed[0:number_of // 2 * 2:2], mixed[1:number_of // 2 * 2:2]
    room = jnp.minimum(tallies[donor] - 1, limit - tallies[sink]) // 2
    room = jnp.where((donor == sequence[0]) | (sink == sequence[0]) | (tallies[sink] == 0), 0, jnp.maximum(room, 0))
    passed = jax.random.randint(jax.random.fold_in(own, 4), (number_of // 2,), 0, 1 << 20) % (room + 1)
    tallies = tallies.at[donor].add(-passed).at[sink].add(passed)
    members = jnp.searchsorted(jnp.cumsum(tallies), jnp.arange(rows * top), side="right").astype(jnp.int32)
    listing = members.reshape(top, rows).T
    listing = listing[jax.random.permutation(jax.random.fold_in(own, 1), rows)]
    rotation = jax.random.randint(jax.random.fold_in(own, 2), (rows, 1), 0, top)
    return jnp.take_along_axis(listing, (jnp.arange(top)[None, :] + rotation) % top, axis=1)


def load_shares(number_of, total, reach, slope, full):
    weights = [(1 << 20) // math.isqrt(grade ** slope) + 1 for grade in range(1, number_of + 1)]
    largest = reach if full else min(reach, max(-(-total // number_of), total * weights[0] // sum(weights)))
    least = 1 if total - largest >= number_of - 1 else 0
    given, rest = [largest] + [least] * (number_of - 1), total - largest - least * (number_of - 1)
    while rest > 0:
        movable = [i for i in range(1, number_of) if given[i] < largest] or [i for i in range(1, number_of) if given[i] < reach]
        whole, left = sum([weights[i] for i in movable]), rest
        for i in movable:
            more = min(reach - given[i], max(1, left * weights[i] // whole), rest)
            given[i] = given[i] + more
            rest = rest - more
    return np.array(given)


def normal_values(stream_key, dims, deviation, limit, cuts=(), kind=jnp.bfloat16):
    values = deviation * jax.random.normal(stream_key, dims, jnp.float32)
    if cuts:
        values = values * block_levels(stream_key, dims, cuts, -0.22, 0.18)
    return jnp.clip(values, -limit, limit).astype(kind)


def setup_inputs(seed: int = 0) -> dict:
    arg_keys = jax.random.split(jax.random.key(seed), 17)
    lru_input = draw_lru_input(jax.random.fold_in(arg_keys[16], 71), 0)
    gate_input = normal_values(arg_keys[1], (TOKENS, D_RNN), 1.0, 6.0, ((0, 4), (1, 8)))
    documents = jnp.searchsorted(jnp.cumsum(ragged_sizes(arg_keys[2], DOCS, TOKENS, DOC_MOST, 0)), jnp.arange(TOKENS), side="right").astype(jnp.int32)
    conv_taps = normal_values(arg_keys[3], (CONV_TAPS, D_RNN), CONV_TAPS ** -0.5, 3.0, ((1, 8),))
    rate_weight = normal_values(arg_keys[4], (LRU_BLOCKS, LRU_BLOCK, LRU_BLOCK), LRU_BLOCK ** -0.5, 0.5, ((0, 8),))
    inlet_weight = normal_values(arg_keys[5], (LRU_BLOCKS, LRU_BLOCK, LRU_BLOCK), LRU_BLOCK ** -0.5, 0.5, ((0, 8),))
    decay_param = draw_decay_param(jax.random.fold_in(arg_keys[16], 71), 0)
    lru_gain = jnp.clip(1.0 + 0.18 * jax.random.normal(arg_keys[7], (D_RNN,), jnp.float32), 0.1, 1.9)
    out_weight = normal_values(arg_keys[8], (D_RNN, D), D_RNN ** -0.5, 0.125, ((0, 8),))
    residual = normal_values(arg_keys[9], (TOKENS, D), 1.0, 6.0, ((0, 4),))
    ffn_gain = jnp.clip(1.0 + 0.18 * jax.random.normal(arg_keys[10], (D,), jnp.float32), 0.1, 1.9)
    routes_keys = jax.random.split(jax.random.fold_in(arg_keys[11], 1), TOKENS // ROUTE_ROWS)
    routes_turns = jax.random.permutation(jax.random.fold_in(arg_keys[11], 3), TOKENS // ROUTE_ROWS)
    routes = jax.vmap(lambda own, number: deal_out(jax.random.fold_in(arg_keys[11], 2), own, number, ROUTE_ROWS, EXPERTS, TOP, CAP, 2))(routes_keys, routes_turns).reshape((TOKENS, TOP))
    route_weights = jnp.clip(0.1 + 0.79999997 * jax.random.uniform(arg_keys[12], (TOKENS, TOP), jnp.float32) ** block_levels(arg_keys[12], (TOKENS, TOP), ((0, 4),), -0.2, 0.2), 0.1, 0.9)
    w_gate = normal_values(arg_keys[13], (EXPERTS, D, FF), D ** -0.5, 0.125, ((0, 4), (2, 8)))
    w_up = normal_values(arg_keys[14], (EXPERTS, D, FF), D ** -0.5, 0.125, ((0, 4), (2, 8)))
    w_down = normal_values(arg_keys[15], (EXPERTS, FF, D), FF ** -0.5, 0.078125, ((0, 4), (1, 8)))
    return {"lru_input": lru_input, "gate_input": gate_input, "documents": documents, "conv_taps": conv_taps, "rate_weight": rate_weight, "inlet_weight": inlet_weight, "decay_param": decay_param, "lru_gain": lru_gain, "out_weight": out_weight, "residual": residual, "ffn_gain": ffn_gain, "routes": routes, "route_weights": route_weights, "w_gate": w_gate, "w_up": w_up, "w_down": w_down}


EPSILON = 1e-06
RATE_SCALE = 8.0

def join_runs(earlier_run, later_run):
    return (earlier_run[0] * later_run[0], later_run[0] * earlier_run[1] + later_run[1])

def slot_targets(route_block, expert_count, capacity):
    flat_routes = route_block.reshape(-1)
    onehot = (flat_routes[:, None] == jnp.arange(expert_count, dtype=jnp.int32)[None, :]).astype(jnp.int32)
    earlier_hits = jnp.cumsum(onehot, axis=0) - onehot
    slot_index = lax.optimization_barrier(jnp.sum(earlier_hits * onehot, axis=1))
    return (flat_routes * capacity + slot_index).astype(jnp.int32).reshape(route_block.shape)

def rms_rows(row_block, gain_vector):
    floated = row_block.astype(jnp.float32)
    inverse_rms = lax.rsqrt(lax.optimization_barrier(jnp.mean(floated * floated, axis=1, keepdims=True)) + EPSILON)
    return (floated * inverse_rms * gain_vector.astype(jnp.float32)[None, :]).astype(jnp.bfloat16)

def summed_blocks(left_rows, right_rows, blocks):
    span_width = left_rows.shape[1] // blocks

    def add_block(running, block_index):
        start_col = (block_index * span_width).astype(jnp.int32)
        partial_sum = jnp.dot(lax.dynamic_slice_in_dim(left_rows, start_col, span_width, 1), lax.dynamic_slice_in_dim(right_rows, start_col, span_width, 0), preferred_element_type=jnp.float32)
        partial_sum = lax.optimization_barrier(partial_sum.astype(jnp.bfloat16)).astype(jnp.float32)
        return (running + partial_sum, None)
    running, _ = lax.scan(add_block, jnp.zeros((left_rows.shape[0], right_rows.shape[1]), jnp.float32), jnp.arange(blocks, dtype=jnp.int32))
    return running

def reference(lru_input, gate_input, documents, conv_taps, rate_weight, inlet_weight, decay_param, lru_gain, out_weight, residual, ffn_gain, routes, route_weights, w_gate, w_up, w_down):
    documents = documents.astype(jnp.int32)
    reach_back = CONV_TAPS - 1
    prior_docs = jnp.concatenate([jnp.full((reach_back,), -1, jnp.int32), documents])
    padded_input = jnp.concatenate([jnp.zeros((reach_back, D_RNN), jnp.bfloat16), lru_input], axis=0)
    conv_sum = jnp.zeros((TOKENS, D_RNN), jnp.float32)
    for tap_index in range(CONV_TAPS):
        same_doc = (prior_docs[tap_index:tap_index + TOKENS] == documents).astype(jnp.float32)[:, None]
        conv_sum = conv_sum + padded_input[tap_index:tap_index + TOKENS].astype(jnp.float32) * conv_taps[tap_index].astype(jnp.float32)[None, :] * same_doc
    convolved = conv_sum.astype(jnp.bfloat16)
    grouped = convolved.astype(jnp.float32).reshape(TOKENS, LRU_BLOCKS, LRU_BLOCK)
    rate_gate = jax.nn.sigmoid(jnp.einsum('tnc,ncd->tnd', grouped, rate_weight.astype(jnp.float32)).reshape(TOKENS, D_RNN))
    inlet_gate = jax.nn.sigmoid(jnp.einsum('tnc,ncd->tnd', grouped, inlet_weight.astype(jnp.float32)).reshape(TOKENS, D_RNN))
    log_decay = -RATE_SCALE * rate_gate * jax.nn.softplus(-decay_param.astype(jnp.float32))[None, :]
    starts = (prior_docs[reach_back - 1:reach_back - 1 + TOKENS] != documents)[:, None]
    decay_step = jnp.where(starts, 0.0, jnp.exp(log_decay))
    norm_factor = jnp.where(starts, 1.0, jnp.sqrt(-jnp.expm1(2.0 * log_decay)))
    drive_term = norm_factor * inlet_gate * convolved.astype(jnp.float32)
    _, hidden_state = lax.associative_scan(join_runs, (decay_step, drive_term), axis=0)
    inverse_rms = lax.rsqrt(lax.optimization_barrier(jnp.mean(hidden_state * hidden_state, axis=1, keepdims=True)) + EPSILON)
    mixer_rows = (hidden_state * inverse_rms * lru_gain.astype(jnp.float32)[None, :] * jax.nn.gelu(gate_input.astype(jnp.float32))).astype(jnp.bfloat16)
    projected = summed_blocks(mixer_rows, out_weight, N_TP)
    after_mixer = (residual.astype(jnp.float32) + projected).astype(jnp.bfloat16)
    normed = rms_rows(after_mixer, ffn_gain)
    block_count = TOKENS // ROUTE_ROWS
    route_blocks = routes.astype(jnp.int32).reshape(block_count, ROUTE_ROWS, TOP)

    def block_slots(route_block):
        return slot_targets(route_block, EXPERTS, CAP)
    targets = jax.vmap(block_slots)(route_blocks)
    slot_index = targets - route_blocks * CAP
    block_ids = jnp.arange(block_count, dtype=jnp.int32)[:, None, None]
    buffer_rows = ((route_blocks * block_count + block_ids) * CAP + slot_index).astype(jnp.int32).reshape(-1)
    token_ids = jnp.broadcast_to(jnp.arange(TOKENS, dtype=jnp.int32).reshape(block_count, ROUTE_ROWS, 1), route_blocks.shape).reshape(-1)
    slot_table = jnp.zeros((EXPERTS * block_count * CAP,), jnp.int32).at[buffer_rows].set(token_ids + 1)
    padded_normed = jnp.concatenate([jnp.zeros((1, D), jnp.bfloat16), normed], axis=0)
    expert_span = block_count * CAP

    def run_expert(expert_id):
        picked_ids = lax.dynamic_slice_in_dim(slot_table, (expert_id * expert_span).astype(jnp.int32), expert_span, 0)
        expert_in = padded_normed[picked_ids]
        gate_part = jnp.dot(expert_in, w_gate[expert_id], preferred_element_type=jnp.float32)
        up_part = jnp.dot(expert_in, w_up[expert_id], preferred_element_type=jnp.float32)
        hidden_units = (jax.nn.silu(gate_part) * up_part).astype(jnp.bfloat16)
        return summed_blocks(hidden_units, w_down[expert_id], N_TP).astype(jnp.bfloat16)
    expert_out = lax.map(run_expert, jnp.arange(EXPERTS, dtype=jnp.int32))
    gathered = expert_out.reshape(EXPERTS * expert_span, D)[buffer_rows].astype(jnp.float32).reshape(TOKENS, TOP, D)
    routed = lax.optimization_barrier(jnp.sum(gathered * route_weights.astype(jnp.float32)[:, :, None], axis=1))
    return (after_mixer.astype(jnp.float32) + routed).astype(jnp.bfloat16)
```

```python
import functools

import jax
import jax.numpy as jnp
from jax import lax
from jax.experimental import pallas as pl
from jax.experimental.pallas import tpu as pltpu
from jax.sharding import PartitionSpec as P

D_RNN = 2048


EPSILON = 1e-06
RATE_SCALE = 8.0


def shifted(block, axis, distance):
    devices = range(lax.axis_size(axis))
    route = [(i - distance, i) for i in devices if i - distance in devices]
    return lax.ppermute(block, axis, route)


def carried_in(value, axis, join, neutral):
    count, mine = (lax.axis_size(axis), lax.axis_index(axis))
    pieces = jax.tree.map(lambda part: lax.all_gather(part, axis), value)
    so_far = jax.tree.map(
        lambda part, zero: jnp.full_like(part, 0) + jnp.asarray(zero, part.dtype), value, neutral
    )

    def hop(position, so_far):
        longer = join(so_far, jax.tree.map(lambda part: part[position], pieces))
        return jax.tree.map(lambda new, old: jnp.where(position < mine, new, old), longer, so_far)

    return lax.fori_loop(0, count - 1, hop, so_far)


def join_runs(earlier_run, later_run):
    return (earlier_run[0] * later_run[0], later_run[0] * earlier_run[1] + later_run[1])


def slot_targets(route_block, expert_count, capacity):
    flat_routes = route_block.reshape(-1)
    onehot = (flat_routes[:, None] == jnp.arange(expert_count, dtype=jnp.int32)[None, :]).astype(
        jnp.int32
    )
    earlier_hits = jnp.cumsum(onehot, axis=0) - onehot
    slot_index = jnp.sum(earlier_hits * onehot, axis=1)
    return (flat_routes * capacity + slot_index).reshape(route_block.shape)


def pick_matrix(targets, slot_total):
    slot_hits = targets[None, :, :] == jnp.arange(slot_total, dtype=jnp.int32)[:, None, None]
    return jnp.sum(slot_hits.astype(jnp.int32), axis=2).astype(jnp.bfloat16)


def rms_rows(row_block, gain_vector):
    floated = row_block.astype(jnp.float32)
    inverse_rms = lax.rsqrt(jnp.mean(floated * floated, axis=1, keepdims=True) + EPSILON)
    return (floated * inverse_rms * gain_vector[None, :]).astype(jnp.bfloat16)


def expert_apply(row_piece, gate_weight, up_weight, down_weight):
    gate_part = jnp.dot(row_piece, gate_weight, preferred_element_type=jnp.float32)
    up_part = jnp.dot(row_piece, up_weight, preferred_element_type=jnp.float32)
    hidden_units = (jax.nn.silu(gate_part) * up_part).astype(jnp.bfloat16)
    return jnp.dot(hidden_units, down_weight, preferred_element_type=jnp.float32)


def local(
    lru_input,
    gate_input,
    documents,
    conv_taps,
    rate_weight,
    inlet_weight,
    decay_param,
    lru_gain,
    out_weight,
    residual,
    ffn_gain,
    routes,
    route_weights,
    w_gate,
    w_up,
    w_down,
):
    positions = lru_input.shape[0]
    channels = lru_input.shape[1]
    model_width = residual.shape[1]
    reach_back = conv_taps.shape[0] - 1
    tail_rows, tail_docs = shifted(
        (lru_input[positions - reach_back :], documents[positions - reach_back :] + 1), "sp", 1
    )
    prior_docs = jnp.concatenate([tail_docs - 1, documents])
    padded_input = jnp.concatenate([tail_rows, lru_input], axis=0)
    conv_sum = jnp.zeros((positions, channels), jnp.float32)
    for tap_index in range(reach_back + 1):
        same_doc = (prior_docs[tap_index : tap_index + positions] == documents).astype(jnp.float32)[
            :, None
        ]
        conv_sum = (
            conv_sum
            + padded_input[tap_index : tap_index + positions].astype(jnp.float32)
            * conv_taps[tap_index].astype(jnp.float32)[None, :]
            * same_doc
        )
    convolved = conv_sum.astype(jnp.bfloat16)
    grouped = convolved.reshape(positions, rate_weight.shape[0], rate_weight.shape[1])
    rate_gate = jax.nn.sigmoid(
        jnp.einsum(
            "tnc,ncd->tnd", grouped, rate_weight, preferred_element_type=jnp.float32
        ).reshape(positions, channels)
    )
    inlet_gate = jax.nn.sigmoid(
        jnp.einsum(
            "tnc,ncd->tnd", grouped, inlet_weight, preferred_element_type=jnp.float32
        ).reshape(positions, channels)
    )
    log_decay = -RATE_SCALE * rate_gate * jax.nn.softplus(-decay_param)[None, :]
    starts = (prior_docs[reach_back - 1 : reach_back - 1 + positions] != documents)[:, None]
    decay_step = jnp.where(starts, 0.0, jnp.exp(log_decay))
    norm_factor = jnp.where(starts, 1.0, jnp.sqrt(-jnp.expm1(2.0 * log_decay)))
    drive_term = norm_factor * inlet_gate * convolved.astype(jnp.float32)
    decay_run, local_state = lax.associative_scan(join_runs, (decay_step, drive_term), axis=0)
    carried = carried_in(
        (decay_run[positions - 1], local_state[positions - 1]),
        "sp",
        join_runs,
        (jnp.ones((channels,), jnp.float32), jnp.zeros((channels,), jnp.float32)),
    )
    hidden_state = local_state + decay_run * carried[1][None, :]
    square_sums = lax.psum(jnp.sum(hidden_state * hidden_state, axis=1), "tp")
    inverse_rms = lax.rsqrt(square_sums[:, None] / D_RNN + EPSILON)
    mixer_rows = (
        hidden_state * inverse_rms * lru_gain[None, :] * jax.nn.gelu(gate_input.astype(jnp.float32))
    ).astype(jnp.bfloat16)
    tp_count = lax.axis_size("tp")
    tp_here = lax.axis_index("tp")
    expert_count = lax.axis_size("sp")
    route_rows = positions // tp_count
    top_count = routes.shape[1]
    capacity = 2 * top_count * route_rows // expert_count
    slot_total = expert_count * capacity
    projected = lax.psum_scatter(
        jnp.dot(mixer_rows, out_weight, preferred_element_type=jnp.float32).astype(jnp.bfloat16),
        "tp",
        scatter_dimension=0,
        tiled=True,
    ).astype(jnp.float32)
    own_rows = (
        lax.dynamic_slice_in_dim(residual, tp_here * route_rows, route_rows, 0).astype(jnp.float32)
        + projected
    ).astype(jnp.bfloat16)
    own_routes = lax.dynamic_slice_in_dim(routes, tp_here * route_rows, route_rows, 0)
    targets = slot_targets(own_routes, expert_count, capacity)
    outgoing = jnp.dot(
        pick_matrix(targets, slot_total),
        rms_rows(own_rows, ffn_gain),
        preferred_element_type=jnp.float32,
    ).astype(jnp.bfloat16)
    arrived = lax.all_to_all(
        outgoing.reshape(expert_count, capacity, model_width),
        "sp",
        split_axis=0,
        concat_axis=0,
        tiled=True,
    )
    partial_out = expert_apply(
        lax.all_gather(arrived.reshape(slot_total, model_width), "tp", axis=0, tiled=True),
        w_gate[0],
        w_up[0],
        w_down[0],
    )
    expert_out = lax.psum_scatter(
        partial_out.astype(jnp.bfloat16), "tp", scatter_dimension=0, tiled=True
    )
    returned = lax.all_to_all(
        expert_out.reshape(expert_count, capacity, model_width),
        "sp",
        split_axis=0,
        concat_axis=0,
        tiled=True,
    )
    picked = returned.reshape(slot_total, model_width)[targets.reshape(-1)].astype(jnp.float32)
    picked = picked.reshape(route_rows, top_count, model_width)
    own_weights = lax.dynamic_slice_in_dim(route_weights, tp_here * route_rows, route_rows, 0)
    routed = jnp.sum(picked * own_weights[:, :, None], axis=1)
    return (own_rows.astype(jnp.float32) + routed).astype(jnp.bfloat16)


MESH = pl.DeviceIdType.MESH
LANES = 128
GELU_SCALE = 0.7978845608028654


def sender(source, target, send_sem, recv_sem, peer):
    return pltpu.make_async_remote_copy(
        src_ref=source,
        dst_ref=target,
        send_sem=send_sem,
        recv_sem=recv_sem,
        device_id=peer,
        device_id_type=MESH,
    )


def greet(peers):
    barrier = pltpu.get_barrier_semaphore()
    for peer in peers:
        pl.semaphore_signal(barrier, inc=1, device_id=peer, device_id_type=MESH)
    pl.semaphore_wait(barrier, len(peers))


def one_minus_exp(value):
    series = 1.0 + value * (1.0 / 6.0)
    for order in (5.0, 4.0, 3.0, 2.0):
        series = 1.0 + value * (1.0 / order) * series
    return jnp.where(value > -0.25, -value * series, 1.0 - jnp.exp(value))


def down_by(block, distance, filler):
    count = block.shape[0]
    if distance % 8 == 0:
        top = jnp.full((distance, block.shape[1]), filler, block.dtype)
        return jnp.concatenate([top, block[: count - distance]], axis=0)
    row = lax.broadcasted_iota(jnp.int32, block.shape, 0)
    return jnp.where(row >= distance, pltpu.roll(block, distance, 0), filler)


LATE = 8


def layer_kernel(
    n_sp,
    n_tp,
    lru_hbm,
    gate_hbm,
    docs_hbm,
    taps_hbm,
    rate_hbm,
    inlet_hbm,
    decay_hbm,
    gain_hbm,
    out_w_hbm,
    residual_hbm,
    ffn_hbm,
    routes_hbm,
    shares_hbm,
    w_gate_hbm,
    w_up_hbm,
    w_down_hbm,
    out_ref,
    lru_ref,
    gate_ref,
    docs_row,
    taps_ref,
    rate_ref,
    inlet_ref,
    decay_ref,
    gain_ref,
    out_w_ref,
    ffn_ref,
    routes_ref,
    route_w_ref,
    docs_ref,
    weights_ref,
    edge_out,
    edge_in,
    mark_out,
    mark_in,
    carry_out,
    carry_in,
    head_a,
    head_b,
    share_in,
    run_a,
    run_b,
    parts,
    pair_in,
    z_out,
    z_in,
    z_sum,
    z_across,
    squares,
    square_pair,
    square_out,
    square_in,
    res_rows,
    own_ref,
    normed_ref,
    w_gate,
    w_up,
    w_down,
    share_cols,
    blocks,
    hidden_units,
    products,
    back_in,
    joined,
    first_x,
    first_y,
    second_x,
    second_y,
    relay_a,
    relay_b,
    column,
    last_in,
    load_sem,
    res_sem,
    w_sem,
    own_sem,
    edge_s,
    edge_r,
    mark_s,
    mark_r,
    carry_s,
    carry_r,
    share_s,
    share_r,
    pair_s,
    pair_r,
    z_s,
    z_r,
    sq_s,
    sq_r,
    gz_s,
    gz_r,
    gxy_s,
    gxy_r,
    gd_s,
    gd_r,
    gp_s,
    gp_r,
    rp_s,
    rp_r,
    r1_s,
    r1_r,
    r2_s,
    r2_r,
    rz_s,
    rz_r,
):
    me_s, me_t = lax.axis_index("sp"), lax.axis_index("tp")
    n_z = n_tp // 2
    me_z, me_c = me_t // 2, me_t % 2
    rows, channels = lru_ref.shape
    width = out_w_ref.shape[1]
    piece = rows // n_tp
    pairs = (
        (lru_hbm, lru_ref),
        (docs_hbm, docs_row),
        (taps_hbm, taps_ref),
        (rate_hbm, rate_ref),
        (inlet_hbm, inlet_ref),
        (decay_hbm, decay_ref),
        (routes_hbm, routes_ref),
        (shares_hbm, route_w_ref),
        (out_w_hbm, out_w_ref),
        (gate_hbm, gate_ref),
        (gain_hbm, gain_ref),
        (ffn_hbm, ffn_ref),
    )
    loads = [
        pltpu.make_async_copy(source, target, load_sem.at[k])
        for k, (source, target) in enumerate(pairs)
    ]
    for copy in loads:
        copy.start()
    residual_copy = pltpu.make_async_copy(
        residual_hbm.at[pl.ds(pl.multiple_of(me_t * piece, piece), piece)], res_rows, res_sem
    )
    residual_copy.start()
    w_loads = [
        pltpu.make_async_copy(source, target, w_sem.at[k])
        for k, (source, target) in enumerate(
            ((w_gate_hbm, w_gate), (w_up_hbm, w_up), (w_down_hbm, w_down))
        )
    ]
    s_x = me_s + 1 - 2 * (me_s % 2)
    s_y = (me_s + 2) % n_sp
    s_d = n_sp - 1 - me_s
    x_peer, y_peer = (s_x, me_t), (s_y, me_t)
    partner = (me_s, me_z * 2 + 1 - me_c)
    sp_peers = [((me_s + k) % n_sp, me_t) for k in range(1, n_sp)]
    z_near, z_far = me_z + 1 - 2 * (me_z % 2), n_z - 1 - me_z
    upper_side = me_z // 2
    across = (me_z, z_near, 2 - upper_side, 3 - 3 * upper_side)
    middle = (me_z + 1) // 2 % 2 == 1
    outer = (me_z + 1) // 2 % 2 == 0
    near, over = (me_s, z_near * 2 + me_c), (me_s, z_far * 2 + me_c)
    z_peers = [(me_s, across[k] * 2 + me_c) for k in range(1, n_z)]
    greeted = sp_peers + z_peers + [partner]
    barrier = pltpu.get_barrier_semaphore()
    for peer in greeted:
        pl.semaphore_signal(barrier, inc=1, device_id=peer, device_id_type=MESH)
    for k in range(6):
        loads[k].wait()
    for copy in w_loads:
        copy.start()
    docs = jnp.transpose(jnp.broadcast_to(docs_row[...], (8, rows)))
    docs = jnp.broadcast_to(docs[:, :1], (rows, LANES))
    docs_ref[...] = docs
    lane8 = lax.broadcasted_iota(jnp.int32, (8, LANES), 1)
    mark_out[...] = jnp.where(lane8 == 0, docs[:8], docs[rows - 8 :])
    edge_out[0:16] = lru_ref[0:16]
    edge_out[16:32] = lru_ref[rows - 16 :]
    taps = taps_ref[...].astype(jnp.float32)
    reach = taps.shape[0] - 1

    def gates(convolved, starts, group):
        span = slice(group * LANES, (group + 1) * LANES)
        rate = jax.nn.sigmoid(
            jnp.dot(convolved, rate_ref[group], preferred_element_type=jnp.float32)
        )
        inlet = jax.nn.sigmoid(
            jnp.dot(convolved, inlet_ref[group], preferred_element_type=jnp.float32)
        )
        minus = -decay_ref[:, span]
        soft = jnp.maximum(minus, 0.0) + jnp.log1p(jnp.exp(-jnp.abs(minus)))
        log_decay = -RATE_SCALE * rate * soft
        step = jnp.where(starts, 0.0, jnp.exp(log_decay))
        factor = jnp.where(starts, 1.0, jnp.sqrt(one_minus_exp(2.0 * log_decay)))
        return step, factor * inlet * convolved.astype(jnp.float32)

    body = rows - 8
    starts = docs[7 : 7 + body] != docs[8:]
    for group in range(channels // LANES):
        span = slice(group * LANES, (group + 1) * LANES)
        long = lru_ref[:, span].astype(jnp.float32)
        total = jnp.zeros((body, LANES), jnp.float32)
        for tap in range(reach + 1):
            first = 8 - reach + tap
            same = docs[first : first + body] == docs[8:]
            total = total + jnp.where(same, long[first : first + body], 0.0) * taps[tap : tap + 1, span]
        step, state = gates(total.astype(jnp.bfloat16), starts, group)
        distance = 1
        while distance < body:
            state = state + step * down_by(state, distance, 0.0)
            step = step * down_by(step, distance, 1.0)
            distance *= 2
        run_a[8:, span] = step
        run_b[8:, span] = state
        carry_out[:, span] = jnp.concatenate(
            [step[body - 1 :], state[body - 1 :], jnp.zeros((6, LANES), jnp.float32)], axis=0
        )
    pl.semaphore_wait(barrier, len(greeted))
    carry = []
    for k, peer in enumerate(sp_peers):
        carry += [
            sender(carry_out, carry_in.at[me_s], carry_s.at[k], carry_r.at[k], peer),
            sender(mark_out, mark_in.at[me_s], mark_s.at[k], mark_r.at[k], peer),
            sender(edge_out, edge_in.at[me_s], edge_s.at[k], edge_r.at[k], peer),
        ]
    for copy in carry:
        copy.start()
    carry_in[pl.ds(me_s, 1)] = carry_out[...][None]
    mark_in[pl.ds(me_s, 1)] = mark_out[...][None]
    edge_in[pl.ds(me_s, 1)] = edge_out[...][None]
    loads[6].wait()
    loads[7].wait()
    expert = lax.broadcasted_iota(jnp.int32, weights_ref.shape, 0)
    shares = jnp.zeros(weights_ref.shape, jnp.float32)
    for k in range(routes_ref.shape[0]):
        shares = shares + jnp.where(
            routes_ref[k : k + 1] == expert, route_w_ref[k : k + 1], 0.0
        )
    weights_ref[...] = shares
    share = [
        sender(weights_ref, share_in.at[me_s], share_s.at[k], share_r.at[k], peer)
        for k, peer in enumerate(sp_peers)
    ]
    for copy in share:
        copy.start()
    share_in[pl.ds(me_s, 1)] = shares[None]
    for k in (9, 10, 11):
        loads[k].wait()
    raw = gate_ref[...].astype(jnp.float32)
    gelu = 0.5 * raw * (1.0 + jnp.tanh(GELU_SCALE * (raw + 0.044715 * raw * raw * raw)))
    gelu = gelu * gain_ref[...]
    for copy in carry:
        copy.wait()
    xs, now, prior = [], [], []
    for place in range(n_sp):
        marks = mark_in[place]
        now.append(jnp.broadcast_to(marks[:, 0:1], (8, LANES)))
        if place == 0:
            prior.append(jnp.full((8, LANES), -1, jnp.int32))
        else:
            prior.append(jnp.broadcast_to(mark_in[place - 1][:, 1:2], (8, LANES)))
        xs.append(
            jnp.concatenate(
                [
                    edge_in[max(place - 1, 0)].astype(jnp.float32)[24:],
                    edge_in[place].astype(jnp.float32)[:8],
                ],
                axis=0,
            )
        )
    both = [jnp.concatenate([prior[p], now[p]], axis=0) for p in range(n_sp)]
    head_starts = jnp.concatenate([both[p][7:15] != now[p] for p in range(n_sp)], axis=0)
    in_tile = lax.broadcasted_iota(jnp.int32, (8 * n_sp, LANES), 0) % 8
    for group in range(channels // LANES):
        span = slice(group * LANES, (group + 1) * LANES)
        sums = []
        for place in range(n_sp):
            total = jnp.zeros((8, LANES), jnp.float32)
            for tap in range(reach + 1):
                first = 8 - reach + tap
                same = both[place][first : first + 8] == now[place]
                total = total + (
                    jnp.where(same, xs[place][first : first + 8, span], 0.0)
                    * taps[tap : tap + 1, span]
                )
            sums.append(total)
        step, state = gates(jnp.concatenate(sums, axis=0).astype(jnp.bfloat16), head_starts, group)
        for distance in (1, 2, 4):
            inside = in_tile >= distance
            state = state + step * jnp.where(inside, pltpu.roll(state, distance, 0), 0.0)
            step = step * jnp.where(inside, pltpu.roll(step, distance, 0), 1.0)
        head_a[:, :, span] = step.reshape(n_sp, 8, LANES)
        head_b[:, :, span] = state.reshape(n_sp, 8, LANES)
    carried = jnp.zeros((1, channels), jnp.float32)
    for place in range(n_sp - 1):
        entered = head_b[place][7:] + head_a[place][7:] * carried
        tile = carry_in[place]
        carried = jnp.where(place < me_s, tile[1:2] + tile[0:1] * entered, carried)
    top = head_b[pl.ds(me_s, 1)][0] + head_a[pl.ds(me_s, 1)][0] * carried
    hidden = jnp.concatenate([top, run_b[8:] + run_a[8:] * top[7:]], axis=0)
    row_squares = jnp.sum(hidden * hidden, axis=1, keepdims=True)
    for place in range(n_tp):
        packed = jnp.zeros((8, LANES), jnp.float32)
        for j in range(piece // 8):
            first = place * piece + j * 8
            packed = jnp.where(lane8 == j, row_squares[first : first + 8], packed)
        squares[place] = packed
    loads[LATE].wait()
    mixer = (hidden * gelu).astype(jnp.bfloat16)
    tile_width = min(512, width)
    for first in range(0, width, tile_width):
        span = slice(first, first + tile_width)
        product = jnp.dot(mixer, out_w_ref[:, span], preferred_element_type=jnp.float32)
        parts[:, :, span] = product.astype(jnp.bfloat16).reshape(n_tp, piece, tile_width)

    half = width // 2
    halves = (pl.ds(0, half), pl.ds(half, half))
    pair = []
    for i in (3, 2, 1, 0):
        theirs = across[i] * 2 + 1 - me_c
        pair.append(
            (
                sender(squares.at[theirs], square_pair.at[i], pair_s.at[1, i], pair_r.at[1, i], partner),
                sender(parts.at[theirs], pair_in.at[i], pair_s.at[0, i], pair_r.at[0, i], partner),
            )
        )
        for copy in pair[-1]:
            copy.start()
    square_copies = []
    inward = {}
    for i in (3, 2, 1):
        for h in range(2):
            inward[i, h] = sender(
                z_out.at[i, :, halves[h]], z_in.at[i, :, halves[h]], z_s.at[h, i], z_r.at[h, i], near
            )
    for n, i in enumerate((3, 2, 1, 0)):
        mine = across[i] * 2 + me_c
        for copy in pair[n]:
            copy.wait_recv()
        square_out[i] = squares[mine] + square_pair[i]
        if i > 0:
            copy = sender(
                square_out.at[i], square_in.at[me_z], sq_s.at[i], sq_r.at[me_z], z_peers[i - 1]
            )
            copy.start()
            square_copies.append(copy)
        z_out[i] = (
            parts[mine].astype(jnp.float32) + pair_in[i].astype(jnp.float32)
        ).astype(jnp.bfloat16)

        if i > 0:

            @pl.when(outer)
            def _():
                for h in range(2):
                    inward[i, h].start()

    crossing, outward = {}, {}
    for i in (3, 2):
        for h in range(2):
            crossing[i, h] = sender(
                z_sum.at[i, :, halves[h]], z_across.at[i, :, halves[h]], z_s.at[h, i + 2], z_r.at[h, i + 2], over
            )
    for h in range(2):
        outward[h] = sender(
            z_sum.at[1, :, halves[h]], z_in.at[0, :, halves[h]], z_s.at[h, 0], z_r.at[h, 0], near
        )

    @pl.when(middle)
    def _():
        def add_up(target, i, h, received):
            span = slice(h * half, (h + 1) * half)
            target[i, :, span] = (
                z_out[i, :, span].astype(jnp.float32) + received[:, span].astype(jnp.float32)
            ).astype(jnp.bfloat16)

        for i, h in ((3, 0), (3, 1), (2, 0)):
            inward[i, h].wait_recv()
            add_up(z_sum, i, h, z_in.at[i])
            crossing[i, h].start()
        for h in range(2):
            if h == 1:
                inward[2, 1].wait_recv()
                add_up(z_sum, 2, 1, z_in.at[2])
                crossing[2, 1].start()
            crossing[3, h].wait_recv()
            add_up(z_sum, 1, h, z_across.at[3])
            outward[h].start()
        for h in range(2):
            inward[1, h].wait_recv()
            add_up(z_sum, 0, h, z_in.at[1])
        for h in range(2):
            crossing[2, h].wait_recv()
        z_in[0] = (z_sum[0].astype(jnp.float32) + z_across[2].astype(jnp.float32)).astype(jnp.bfloat16)
        z_sum[0] = z_in[0]

    @pl.when(outer)
    def _():
        for h in range(2):
            outward[h].wait_recv()
        z_sum[0] = (z_out[0].astype(jnp.float32) + z_in[0].astype(jnp.float32)).astype(jnp.bfloat16)

    summed = z_sum[0].astype(jnp.float32)
    square_sum = square_out[0]
    for k in range(1, n_z):
        from_z = (me_z + k) % n_z
        sender(
            square_out.at[0], square_in.at[from_z], sq_s.at[0], sq_r.at[from_z], near
        ).wait_recv()
        square_sum = square_sum + square_in[pl.ds(from_z, 1)][0]
    square_sum = jnp.concatenate(
        [square_sum[:, j : j + 1] for j in range(piece // 8)], axis=0
    )
    inverse = lax.rsqrt(square_sum / (channels * n_tp) + EPSILON)
    residual_copy.wait()
    own = (res_rows[...].astype(jnp.float32) + summed * inverse).astype(jnp.bfloat16)
    own_ref[...] = own
    floated = own.astype(jnp.float32)
    inverse = lax.rsqrt(jnp.mean(floated * floated, axis=1, keepdims=True) + EPSILON)
    normed_ref[...] = (floated * inverse * ffn_ref[...]).astype(jnp.bfloat16)

    lower, upper = halves
    sent = []

    def push(source, target, sems, slot, peer):
        copy = sender(source, target, sems[0].at[slot], sems[1].at[slot], peer)
        copy.start()
        sent.append(copy)
        return copy

    gz, gxy, gd, gp = (gz_s, gz_r), (gxy_s, gxy_r), (gd_s, gd_r), (gp_s, gp_r)
    rp, r1, r2, rz = (rp_s, rp_r), (r1_s, r1_r), (r2_s, r2_r), (rz_s, rz_r)
    from_x, from_y, from_da, from_db, from_pair = {}, {}, {}, {}, {}
    mid_sent = []

    def arrival(i):
        block = blocks.at[i, me_s, me_c]
        return sender(block, block, gz[0].at[i], gz[1].at[i], near)

    def mid_push(source, i, slot, peer):
        copy = sender(source, blocks.at[i, me_s, me_c], gz[0].at[slot], gz[1].at[i], peer)
        pl.when(middle)(copy.start)
        mid_sent.append(copy)

    def pass_on(i):
        pl.when(middle)(arrival(i).wait_recv)
        mid_push(blocks.at[i, me_s, me_c], i, i + 2, near)

    def spread(i):
        block = blocks.at[i, me_s, me_c]
        if i == 0:
            source = normed_ref
        elif i == 1:
            arrival(1).wait_recv()
            source = block
        else:
            pl.when(outer)(arrival(i).wait_recv)
            source = block
        for h in range(2):
            part, other = halves[h], halves[1 - h]
            from_x[h, i] = push(source.at[:, part], block.at[:, part], gxy, (h, i), x_peer)
            from_y[1 - h, i] = push(source.at[:, other], block.at[:, other], gxy, (3 - h, i), y_peer)
        if i == 0:
            sent.append(sender(source, blocks.at[1, me_s, me_c], gz[0].at[1], gz[1].at[1], near))
            sent[-1].start()
            mid_push(source, 2, 2, over)
        elif i == 1:
            mid_push(source, 3, 3, over)
        from_pair[0, i] = push(source, block, gp, (0, i), partner)

    def relay(i):
        from_x[0, i].wait_recv()
        part = blocks.at[i, s_x, me_c, :, lower]
        from_da[i] = push(part, part, gd, (0, i), y_peer)
        from_y[1, i].wait_recv()
        part = blocks.at[i, s_y, me_c, :, upper]
        from_db[i] = push(part, part, gd, (1, i), x_peer)

    def share_xy(i):
        from_x[1, i].wait_recv()
        block = blocks.at[i, s_x, me_c]
        from_pair[1, i] = push(block, block, gp, (1, i), partner)
        from_y[0, i].wait_recv()
        block = blocks.at[i, s_y, me_c]
        from_pair[2, i] = push(block, block, gp, (2, i), partner)

    def hand_over(i):
        from_da[i].wait_recv()
        part = blocks.at[i, s_d, me_c, :, lower]
        from_pair[3, i] = push(part, part, gp, (3, i), partner)
        from_db[i].wait_recv()
        part = blocks.at[i, s_d, me_c, :, upper]
        from_pair[4, i] = push(part, part, gp, (4, i), partner)

    own_copy = pltpu.make_async_copy(normed_ref, blocks.at[0, me_s, me_c], own_sem)
    own_copy.start()
    spread(0)
    for copy in share:
        copy.wait()
    for place in range(n_sp):
        turned = jnp.transpose(share_in[place])
        lane = lax.broadcasted_iota(jnp.int32, turned.shape, 1)
        chosen = jnp.sum(jnp.where(lane == me_s, turned, 0.0), axis=1, keepdims=True)
        share_cols[place] = jnp.broadcast_to(chosen, (rows, LANES))

    ff = w_gate.shape[1]
    f_tile, d_tile = 256, min(512, width)
    count = n_sp * 2 * piece
    back, first_xs, first_ys, second_xs, second_ys = {}, {}, {}, {}, {}

    def rise(i, step):
        if step == 0:
            for k in range(5):
                from_pair[k, i].wait_recv()
        tokens = blocks[i].reshape(count, width)
        span = slice(step * f_tile, (step + 1) * f_tile)
        gate_part = jnp.dot(tokens, w_gate[:, span], preferred_element_type=jnp.float32)
        up_part = jnp.dot(tokens, w_up[:, span], preferred_element_type=jnp.float32)
        hidden_units[:, span] = (gate_part * jax.nn.sigmoid(gate_part) * up_part).astype(
            jnp.bfloat16
        )

    targets = (s_d, s_x, s_y, me_s)

    def fall(i, h):
        z = across[i]
        first = pl.multiple_of(z * (2 * piece), 2 * piece)
        scale = share_cols[:, pl.ds(first, 2 * piece), :].reshape(count, LANES)[:, :1]
        units = hidden_units[...]
        for step in range(half // d_tile):
            begin = h * half + step * d_tile
            span = slice(begin, begin + d_tile)
            product = jnp.dot(units, w_down[:, span], preferred_element_type=jnp.float32) * scale
            products[i, :, :, :, span] = product.astype(jnp.bfloat16).reshape(
                n_sp, 2, piece, d_tile
            )
        for k, group in enumerate(targets):
            back[k, h, i] = push(
                products.at[i, group, 1 - me_c, :, halves[h]],
                back_in.at[i, k, :, halves[h]],
                rp,
                (h * 4 + k, i),
                partner,
            )

    def merge(i, k, h):
        span = slice(h * half, (h + 1) * half)
        back[k, h, i].wait_recv()
        joined[i, k, :, span] = (
            products[i, targets[k], me_c, :, span].astype(jnp.float32)
            + back_in[i, k, :, span].astype(jnp.float32)
        ).astype(jnp.bfloat16)

    def join(i):
        merge(i, 0, 0)
        first_xs[1, i] = push(joined.at[i, 0, :, lower], first_x.at[1, i], r1, (2, i), x_peer)
        merge(i, 0, 1)
        first_ys[1, i] = push(joined.at[i, 0, :, upper], first_y.at[1, i], r1, (3, i), y_peer)
        merge(i, 1, 0)
        first_xs[0, i] = push(joined.at[i, 1, :, lower], first_x.at[0, i], r1, (0, i), x_peer)
        merge(i, 2, 1)
        first_ys[0, i] = push(joined.at[i, 2, :, upper], first_y.at[0, i], r1, (1, i), y_peer)
        for k, h in ((2, 0), (1, 1), (3, 0), (3, 1)):
            merge(i, k, h)

    def turn(i):
        first_xs[1, i].wait_recv()
        relay_a[i] = (
            joined[i, 2, :, :half].astype(jnp.float32) + first_x[1, i].astype(jnp.float32)
        ).astype(jnp.bfloat16)
        second_ys[i] = push(relay_a.at[i], second_y.at[i], r2, (0, i), y_peer)
        first_ys[1, i].wait_recv()
        relay_b[i] = (
            joined[i, 1, :, half:].astype(jnp.float32) + first_y[1, i].astype(jnp.float32)
        ).astype(jnp.bfloat16)
        second_xs[i] = push(relay_b.at[i], second_x.at[i], r2, (1, i), x_peer)

    def finish(i):
        for copies in (first_xs, first_ys):
            copies[0, i].wait_recv()
        for copies in (second_xs, second_ys):
            copies[i].wait_recv()
        low = (
            joined[i, 3, :, :half].astype(jnp.float32)
            + first_x[0, i].astype(jnp.float32)
            + second_y[i].astype(jnp.float32)
        )
        high = (
            joined[i, 3, :, half:].astype(jnp.float32)
            + first_y[0, i].astype(jnp.float32)
            + second_x[i].astype(jnp.float32)
        )
        column[i] = jnp.concatenate([low, high], axis=1).astype(jnp.bfloat16)
        if i > 0:
            peer = z_peers[i - 1]
            copy = sender(column.at[i], last_in.at[me_z], rz[0].at[i], rz[1].at[me_z], peer)
            copy.start()
            sent.append(copy)

    own_copy.wait()
    for copy in w_loads:
        copy.wait()
    plan = (
        (relay, 0),
        (pass_on, 2),
        (share_xy, 0),
        (spread, 1),
        (hand_over, 0),
        (relay, 1),
        (rise, 0, 0),
        (rise, 0, 1),
        (pass_on, 3),
        (share_xy, 1),
        (spread, 2),
        (rise, 0, 2),
        (fall, 0, 0),
        (hand_over, 1),
        (fall, 0, 1),
        (relay, 2),
        (rise, 1, 0),
        (rise, 1, 1),
        (share_xy, 2),
        (spread, 3),
        (rise, 1, 2),
        (fall, 1, 0),
        (hand_over, 2),
        (fall, 1, 1),
        (relay, 3),
        (rise, 2, 0),
        (rise, 2, 1),
        (share_xy, 3),
        (join, 1),
        (rise, 2, 2),
        (fall, 2, 0),
        (hand_over, 3),
        (fall, 2, 1),
        (turn, 1),
        (rise, 3, 0),
        (rise, 3, 1),
        (join, 2),
        (finish, 1),
        (rise, 3, 2),
        (turn, 2),
        (fall, 3, 0),
        (fall, 3, 1),
        (finish, 2),
        (join, 3),
        (join, 0),
        (turn, 3),
        (finish, 3),
        (turn, 0),
        (finish, 0),
    )
    for stage, *at in plan:
        stage(*at)
    total = own_ref[...].astype(jnp.float32) + column[0].astype(jnp.float32)
    for k in range(1, n_z):
        z = (me_z + k) % n_z
        sender(column.at[0], last_in.at[z], rz[0].at[0], rz[1].at[z], near).wait_recv()
        total = total + last_in[pl.ds(z, 1)][0].astype(jnp.float32)
    out_ref[...] = total.astype(jnp.bfloat16)
    for copies in pair:
        for copy in copies:
            copy.wait_send()
    for copy in square_copies:
        copy.wait_send()

    @pl.when(outer)
    def _():
        for copy in inward.values():
            copy.wait_send()

    @pl.when(middle)
    def _():
        for copy in list(crossing.values()) + list(outward.values()) + mid_sent:
            copy.wait_send()

    for copy in sent:
        copy.wait_send()


def dense_local(
    lru_input,
    gate_input,
    documents,
    conv_taps,
    rate_weight,
    inlet_weight,
    decay_param,
    lru_gain,
    out_weight,
    residual,
    ffn_gain,
    routes,
    route_weights,
    w_gate,
    w_up,
    w_down,
):
    n_sp, n_tp = lax.axis_size("sp"), lax.axis_size("tp")
    n_z = n_tp // 2
    rows, channels = lru_input.shape
    width = residual.shape[1]
    ff = w_gate.shape[2]
    piece = rows // n_tp
    padded = -(-n_sp // 8) * 8
    vmem = pl.BlockSpec(memory_space=pltpu.VMEM)
    half = width // 2
    top = routes.shape[1]
    hbm = pl.BlockSpec(memory_space=pl.ANY)
    bf16, f32 = jnp.bfloat16, jnp.float32
    dma = pltpu.SemaphoreType.DMA
    rows_buffer = pltpu.VMEM((n_z, piece, width), bf16)
    half_buffer = pltpu.VMEM((n_z, piece, half), bf16)
    chunks = pltpu.VMEM((n_z, n_sp, 2, piece, width), bf16)
    groups = pltpu.VMEM((n_z, n_sp, piece, width), bf16)
    square_buffer = pltpu.VMEM((n_z, 8, LANES), f32)
    shapes = (
        [(n_sp,)] * 8
        + [(2, n_z)] * 2
        + [(2, n_z + 2)] * 2
        + [(n_z,)] * 2
        + [(n_z + 2,)] * 2
        + [(4, n_z)] * 2
        + [(2, n_z)] * 2
        + [(5, n_z)] * 2
        + [(8, n_z)] * 2
        + [(4, n_z)] * 2
        + [(2, n_z)] * 2
        + [(n_z,)] * 2
    )
    return pl.pallas_call(
        functools.partial(layer_kernel, n_sp, n_tp),
        out_shape=jax.ShapeDtypeStruct((piece, width), bf16),
        in_specs=[hbm] * 16,
        out_specs=vmem,
        scratch_shapes=[
            pltpu.VMEM((rows, channels), bf16),
            pltpu.VMEM((rows, channels), bf16),
            pltpu.VMEM((1, rows), jnp.int32),
            pltpu.VMEM(conv_taps.shape, bf16),
            pltpu.VMEM(rate_weight.shape, bf16),
            pltpu.VMEM(inlet_weight.shape, bf16),
            pltpu.VMEM((1, channels), f32),
            pltpu.VMEM((1, channels), f32),
            pltpu.VMEM((channels, width), bf16),
            pltpu.VMEM((1, width), f32),
            pltpu.VMEM((top, rows), jnp.int32),
            pltpu.VMEM((top, rows), f32),
            pltpu.VMEM((rows, LANES), jnp.int32),
            pltpu.VMEM((padded, rows), f32),
            pltpu.VMEM((32, channels), bf16),
            pltpu.VMEM((n_sp, 32, channels), bf16),
            pltpu.VMEM((8, LANES), jnp.int32),
            pltpu.VMEM((n_sp, 8, LANES), jnp.int32),
            pltpu.VMEM((8, channels), f32),
            pltpu.VMEM((n_sp, 8, channels), f32),
            pltpu.VMEM((n_sp, 8, channels), f32),
            pltpu.VMEM((n_sp, 8, channels), f32),
            pltpu.VMEM((n_sp, padded, rows), f32),
            pltpu.VMEM((rows, channels), f32),
            pltpu.VMEM((rows, channels), f32),
            pltpu.VMEM((n_tp, piece, width), bf16),
            rows_buffer,
            rows_buffer,
            rows_buffer,
            rows_buffer,
            rows_buffer,
            pltpu.VMEM((n_tp, 8, LANES), f32),
            square_buffer,
            square_buffer,
            square_buffer,
            pltpu.VMEM((piece, width), bf16),
            pltpu.VMEM((piece, width), bf16),
            pltpu.VMEM((piece, width), bf16),
            pltpu.VMEM((width, ff), bf16),
            pltpu.VMEM((width, ff), bf16),
            pltpu.VMEM((ff, width), bf16),
            pltpu.VMEM((n_sp, rows, LANES), f32),
            chunks,
            pltpu.VMEM((n_sp * 2 * piece, ff), bf16),
            chunks,
            groups,
            groups,
            pltpu.VMEM((2, n_z, piece, half), bf16),
            pltpu.VMEM((2, n_z, piece, half), bf16),
            half_buffer,
            half_buffer,
            half_buffer,
            half_buffer,
            rows_buffer,
            rows_buffer,
            dma((12,)),
            dma,
            dma((3,)),
            dma,
        ]
        + [dma(shape) for shape in shapes],
        compiler_params=pltpu.CompilerParams(
            collective_id=0, has_side_effects=True, vmem_limit_bytes=60 * 2**20
        ),
    )(
        lru_input,
        gate_input,
        documents[None, :],
        conv_taps,
        rate_weight,
        inlet_weight,
        decay_param[None, :],
        lru_gain[None, :],
        out_weight,
        residual,
        ffn_gain[None, :],
        routes.T,
        route_weights.T,
        w_gate[0],
        w_up[0],
        w_down[0],
    )


def solution(mesh):
    n_sp, n_tp = mesh.shape["sp"], mesh.shape["tp"]
    body = dense_local if n_sp == 4 and n_tp == 8 else local
    return jax.shard_map(
        body,
        mesh=mesh,
        in_specs=(
            P("sp", "tp"),
            P("sp", "tp"),
            P("sp"),
            P(None, "tp"),
            P("tp", None, None),
            P("tp", None, None),
            P("tp"),
            P("tp"),
            P("tp", None),
            P("sp", None),
            P(),
            P("sp", None),
            P("sp", None),
            P("sp", None, "tp"),
            P("sp", None, "tp"),
            P("sp", "tp", None),
        ),
        out_specs=P(("sp", "tp"), None),
        check_vma=False,
    )
```

```python
import functools

import jax
import jax.numpy as jnp
from jax import lax
from jax.experimental import pallas as pl
from jax.experimental.pallas import tpu as pltpu
from jax.sharding import PartitionSpec as P

D_RNN = 2048


EPSILON = 1e-06
RATE_SCALE = 8.0


def shifted(block, axis, distance):
    devices = range(lax.axis_size(axis))
    route = [(i - distance, i) for i in devices if i - distance in devices]
    return lax.ppermute(block, axis, route)


def carried_in(value, axis, join, neutral):
    count, mine = (lax.axis_size(axis), lax.axis_index(axis))
    pieces = jax.tree.map(lambda part: lax.all_gather(part, axis), value)
    so_far = jax.tree.map(
        lambda part, zero: jnp.full_like(part, 0) + jnp.asarray(zero, part.dtype), value, neutral
    )

    def hop(position, so_far):
        longer = join(so_far, jax.tree.map(lambda part: part[position], pieces))
        return jax.tree.map(lambda new, old: jnp.where(position < mine, new, old), longer, so_far)

    return lax.fori_loop(0, count - 1, hop, so_far)


def join_runs(earlier_run, later_run):
    return (earlier_run[0] * later_run[0], later_run[0] * earlier_run[1] + later_run[1])


def slot_targets(route_block, expert_count, capacity):
    flat_routes = route_block.reshape(-1)
    onehot = (flat_routes[:, None] == jnp.arange(expert_count, dtype=jnp.int32)[None, :]).astype(
        jnp.int32
    )
    earlier_hits = jnp.cumsum(onehot, axis=0) - onehot
    slot_index = jnp.sum(earlier_hits * onehot, axis=1)
    return (flat_routes * capacity + slot_index).reshape(route_block.shape)


def pick_matrix(targets, slot_total):
    slot_hits = targets[None, :, :] == jnp.arange(slot_total, dtype=jnp.int32)[:, None, None]
    return jnp.sum(slot_hits.astype(jnp.int32), axis=2).astype(jnp.bfloat16)


def rms_rows(row_block, gain_vector):
    floated = row_block.astype(jnp.float32)
    inverse_rms = lax.rsqrt(jnp.mean(floated * floated, axis=1, keepdims=True) + EPSILON)
    return (floated * inverse_rms * gain_vector[None, :]).astype(jnp.bfloat16)


def expert_apply(row_piece, gate_weight, up_weight, down_weight):
    gate_part = jnp.dot(row_piece, gate_weight, preferred_element_type=jnp.float32)
    up_part = jnp.dot(row_piece, up_weight, preferred_element_type=jnp.float32)
    hidden_units = (jax.nn.silu(gate_part) * up_part).astype(jnp.bfloat16)
    return jnp.dot(hidden_units, down_weight, preferred_element_type=jnp.float32)


def local(
    lru_input,
    gate_input,
    documents,
    conv_taps,
    rate_weight,
    inlet_weight,
    decay_param,
    lru_gain,
    out_weight,
    residual,
    ffn_gain,
    routes,
    route_weights,
    w_gate,
    w_up,
    w_down,
):
    positions = lru_input.shape[0]
    channels = lru_input.shape[1]
    model_width = residual.shape[1]
    reach_back = conv_taps.shape[0] - 1
    tail_rows, tail_docs = shifted(
        (lru_input[positions - reach_back :], documents[positions - reach_back :] + 1), "sp", 1
    )
    prior_docs = jnp.concatenate([tail_docs - 1, documents])
    padded_input = jnp.concatenate([tail_rows, lru_input], axis=0)
    conv_sum = jnp.zeros((positions, channels), jnp.float32)
    for tap_index in range(reach_back + 1):
        same_doc = (prior_docs[tap_index : tap_index + positions] == documents).astype(jnp.float32)[
            :, None
        ]
        conv_sum = (
            conv_sum
            + padded_input[tap_index : tap_index + positions].astype(jnp.float32)
            * conv_taps[tap_index].astype(jnp.float32)[None, :]
            * same_doc
        )
    convolved = conv_sum.astype(jnp.bfloat16)
    grouped = convolved.reshape(positions, rate_weight.shape[0], rate_weight.shape[1])
    rate_gate = jax.nn.sigmoid(
        jnp.einsum(
            "tnc,ncd->tnd", grouped, rate_weight, preferred_element_type=jnp.float32
        ).reshape(positions, channels)
    )
    inlet_gate = jax.nn.sigmoid(
        jnp.einsum(
            "tnc,ncd->tnd", grouped, inlet_weight, preferred_element_type=jnp.float32
        ).reshape(positions, channels)
    )
    log_decay = -RATE_SCALE * rate_gate * jax.nn.softplus(-decay_param)[None, :]
    starts = (prior_docs[reach_back - 1 : reach_back - 1 + positions] != documents)[:, None]
    decay_step = jnp.where(starts, 0.0, jnp.exp(log_decay))
    norm_factor = jnp.where(starts, 1.0, jnp.sqrt(-jnp.expm1(2.0 * log_decay)))
    drive_term = norm_factor * inlet_gate * convolved.astype(jnp.float32)
    decay_run, local_state = lax.associative_scan(join_runs, (decay_step, drive_term), axis=0)
    carried = carried_in(
        (decay_run[positions - 1], local_state[positions - 1]),
        "sp",
        join_runs,
        (jnp.ones((channels,), jnp.float32), jnp.zeros((channels,), jnp.float32)),
    )
    hidden_state = local_state + decay_run * carried[1][None, :]
    square_sums = lax.psum(jnp.sum(hidden_state * hidden_state, axis=1), "tp")
    inverse_rms = lax.rsqrt(square_sums[:, None] / D_RNN + EPSILON)
    mixer_rows = (
        hidden_state * inverse_rms * lru_gain[None, :] * jax.nn.gelu(gate_input.astype(jnp.float32))
    ).astype(jnp.bfloat16)
    tp_count = lax.axis_size("tp")
    tp_here = lax.axis_index("tp")
    expert_count = lax.axis_size("sp")
    route_rows = positions // tp_count
    top_count = routes.shape[1]
    capacity = 2 * top_count * route_rows // expert_count
    slot_total = expert_count * capacity
    projected = lax.psum_scatter(
        jnp.dot(mixer_rows, out_weight, preferred_element_type=jnp.float32).astype(jnp.bfloat16),
        "tp",
        scatter_dimension=0,
        tiled=True,
    ).astype(jnp.float32)
    own_rows = (
        lax.dynamic_slice_in_dim(residual, tp_here * route_rows, route_rows, 0).astype(jnp.float32)
        + projected
    ).astype(jnp.bfloat16)
    own_routes = lax.dynamic_slice_in_dim(routes, tp_here * route_rows, route_rows, 0)
    targets = slot_targets(own_routes, expert_count, capacity)
    outgoing = jnp.dot(
        pick_matrix(targets, slot_total),
        rms_rows(own_rows, ffn_gain),
        preferred_element_type=jnp.float32,
    ).astype(jnp.bfloat16)
    arrived = lax.all_to_all(
        outgoing.reshape(expert_count, capacity, model_width),
        "sp",
        split_axis=0,
        concat_axis=0,
        tiled=True,
    )
    partial_out = expert_apply(
        lax.all_gather(arrived.reshape(slot_total, model_width), "tp", axis=0, tiled=True),
        w_gate[0],
        w_up[0],
        w_down[0],
    )
    expert_out = lax.psum_scatter(
        partial_out.astype(jnp.bfloat16), "tp", scatter_dimension=0, tiled=True
    )
    returned = lax.all_to_all(
        expert_out.reshape(expert_count, capacity, model_width),
        "sp",
        split_axis=0,
        concat_axis=0,
        tiled=True,
    )
    picked = returned.reshape(slot_total, model_width)[targets.reshape(-1)].astype(jnp.float32)
    picked = picked.reshape(route_rows, top_count, model_width)
    own_weights = lax.dynamic_slice_in_dim(route_weights, tp_here * route_rows, route_rows, 0)
    routed = jnp.sum(picked * own_weights[:, :, None], axis=1)
    return (own_rows.astype(jnp.float32) + routed).astype(jnp.bfloat16)


MESH = pl.DeviceIdType.MESH
LANES = 128
GELU_SCALE = 0.7978845608028654


def sender(source, target, send_sem, recv_sem, peer):
    return pltpu.make_async_remote_copy(
        src_ref=source,
        dst_ref=target,
        send_sem=send_sem,
        recv_sem=recv_sem,
        device_id=peer,
        device_id_type=MESH,
    )


def greet(peers):
    barrier = pltpu.get_barrier_semaphore()
    for peer in peers:
        pl.semaphore_signal(barrier, inc=1, device_id=peer, device_id_type=MESH)
    pl.semaphore_wait(barrier, len(peers))


def one_minus_exp(value):
    series = 1.0 + value * (1.0 / 6.0)
    for order in (5.0, 4.0, 3.0, 2.0):
        series = 1.0 + value * (1.0 / order) * series
    return jnp.where(value > -0.25, -value * series, 1.0 - jnp.exp(value))


def down_by(block, distance, filler):
    count = block.shape[0]
    if distance % 8 == 0:
        top = jnp.full((distance, block.shape[1]), filler, block.dtype)
        return jnp.concatenate([top, block[: count - distance]], axis=0)
    row = lax.broadcasted_iota(jnp.int32, block.shape, 0)
    return jnp.where(row >= distance, pltpu.roll(block, distance, 0), filler)


LATE = 8


def layer_kernel(
    n_sp,
    n_tp,
    lru_hbm,
    gate_hbm,
    docs_hbm,
    taps_hbm,
    rate_hbm,
    inlet_hbm,
    decay_hbm,
    gain_hbm,
    out_w_hbm,
    residual_hbm,
    ffn_hbm,
    routes_hbm,
    shares_hbm,
    w_gate_hbm,
    w_up_hbm,
    w_down_hbm,
    out_ref,
    lru_ref,
    gate_ref,
    docs_row,
    taps_ref,
    rate_ref,
    inlet_ref,
    decay_ref,
    gain_ref,
    out_w_ref,
    ffn_ref,
    routes_ref,
    route_w_ref,
    docs_ref,
    weights_ref,
    edge_out,
    edge_in,
    mark_out,
    mark_in,
    carry_out,
    carry_in,
    head_a,
    head_b,
    share_in,
    run_a,
    run_b,
    parts,
    pair_in,
    z_out,
    z_in,
    z_sum,
    z_across,
    squares,
    square_pair,
    square_out,
    square_in,
    res_rows,
    own_ref,
    normed_ref,
    w_gate,
    w_up,
    w_down,
    share_cols,
    blocks,
    hidden_units,
    joined,
    first_x,
    first_y,
    second_x,
    second_y,
    relay_a,
    relay_b,
    relay_c,
    column,
    last_in,
    load_sem,
    res_sem,
    w_sem,
    own_sem,
    edge_s,
    edge_r,
    mark_s,
    mark_r,
    carry_s,
    carry_r,
    share_s,
    share_r,
    pair_s,
    pair_r,
    z_s,
    z_r,
    sq_s,
    sq_r,
    gz_s,
    gz_r,
    gxy_s,
    gxy_r,
    gd_s,
    gd_r,
    wp_s,
    wp_r,
    r1_s,
    r1_r,
    r2_s,
    r2_r,
    rz_s,
    rz_r,
):
    me_s, me_t = lax.axis_index("sp"), lax.axis_index("tp")
    n_z = n_tp // 2
    me_z, me_c = me_t // 2, me_t % 2
    rows, channels = lru_ref.shape
    width = out_w_ref.shape[1]
    piece = rows // n_tp
    pairs = (
        (lru_hbm, lru_ref),
        (docs_hbm, docs_row),
        (taps_hbm, taps_ref),
        (rate_hbm, rate_ref),
        (inlet_hbm, inlet_ref),
        (decay_hbm, decay_ref),
        (routes_hbm, routes_ref),
        (shares_hbm, route_w_ref),
        (out_w_hbm, out_w_ref),
        (gate_hbm, gate_ref),
        (gain_hbm, gain_ref),
        (ffn_hbm, ffn_ref),
    )
    loads = [
        pltpu.make_async_copy(source, target, load_sem.at[k])
        for k, (source, target) in enumerate(pairs)
    ]
    for copy in loads:
        copy.start()
    residual_copy = pltpu.make_async_copy(
        residual_hbm.at[pl.ds(pl.multiple_of(me_t * piece, piece), piece)], res_rows, res_sem
    )
    residual_copy.start()
    w_loads = [
        pltpu.make_async_copy(source, target, w_sem.at[k])
        for k, (source, target) in enumerate(
            (
                (w_gate_hbm, w_gate.at[me_c]),
                (w_up_hbm, w_up.at[me_c]),
                (w_down_hbm, w_down.at[me_c]),
            )
        )
    ]
    s_x = me_s + 1 - 2 * (me_s % 2)
    s_y = (me_s + 2) % n_sp
    s_d = n_sp - 1 - me_s
    x_peer, y_peer = (s_x, me_t), (s_y, me_t)
    partner = (me_s, me_z * 2 + 1 - me_c)
    sp_peers = [((me_s + k) % n_sp, me_t) for k in range(1, n_sp)]
    z_near, z_far = me_z + 1 - 2 * (me_z % 2), n_z - 1 - me_z
    upper_side = me_z // 2
    across = (me_z, z_near, 2 - upper_side, 3 - 3 * upper_side)
    middle = (me_z + 1) // 2 % 2 == 1
    outer = (me_z + 1) // 2 % 2 == 0
    near, over = (me_s, z_near * 2 + me_c), (me_s, z_far * 2 + me_c)
    z_peers = [(me_s, across[k] * 2 + me_c) for k in range(1, n_z)]
    greeted = sp_peers + z_peers + [partner]
    barrier = pltpu.get_barrier_semaphore()
    for peer in greeted:
        pl.semaphore_signal(barrier, inc=1, device_id=peer, device_id_type=MESH)
    for k in range(6):
        loads[k].wait()
    for copy in w_loads:
        copy.start()
    docs = jnp.transpose(jnp.broadcast_to(docs_row[...], (8, rows)))
    docs = jnp.broadcast_to(docs[:, :1], (rows, LANES))
    docs_ref[...] = docs
    lane8 = lax.broadcasted_iota(jnp.int32, (8, LANES), 1)
    mark_out[...] = jnp.where(lane8 == 0, docs[:8], docs[rows - 8 :])
    edge_out[0:16] = lru_ref[0:16]
    edge_out[16:32] = lru_ref[rows - 16 :]
    taps = taps_ref[...].astype(jnp.float32)
    reach = taps.shape[0] - 1

    def gates(convolved, starts, group):
        span = slice(group * LANES, (group + 1) * LANES)
        rate = jax.nn.sigmoid(
            jnp.dot(convolved, rate_ref[group], preferred_element_type=jnp.float32)
        )
        inlet = jax.nn.sigmoid(
            jnp.dot(convolved, inlet_ref[group], preferred_element_type=jnp.float32)
        )
        minus = -decay_ref[:, span]
        soft = jnp.maximum(minus, 0.0) + jnp.log1p(jnp.exp(-jnp.abs(minus)))
        log_decay = -RATE_SCALE * rate * soft
        step = jnp.where(starts, 0.0, jnp.exp(log_decay))
        factor = jnp.where(starts, 1.0, jnp.sqrt(one_minus_exp(2.0 * log_decay)))
        return step, factor * inlet * convolved.astype(jnp.float32)

    body = rows - 8
    starts = docs[7 : 7 + body] != docs[8:]
    for group in range(channels // LANES):
        span = slice(group * LANES, (group + 1) * LANES)
        long = lru_ref[:, span].astype(jnp.float32)
        total = jnp.zeros((body, LANES), jnp.float32)
        for tap in range(reach + 1):
            first = 8 - reach + tap
            same = docs[first : first + body] == docs[8:]
            total = total + jnp.where(same, long[first : first + body], 0.0) * taps[tap : tap + 1, span]
        step, state = gates(total.astype(jnp.bfloat16), starts, group)
        distance = 1
        while distance < body:
            state = state + step * down_by(state, distance, 0.0)
            step = step * down_by(step, distance, 1.0)
            distance *= 2
        run_a[8:, span] = step
        run_b[8:, span] = state
        carry_out[:, span] = jnp.concatenate(
            [step[body - 1 :], state[body - 1 :], jnp.zeros((6, LANES), jnp.float32)], axis=0
        )
    pl.semaphore_wait(barrier, len(greeted))
    carry = []
    for k, peer in enumerate(sp_peers):
        carry += [
            sender(carry_out, carry_in.at[me_s], carry_s.at[k], carry_r.at[k], peer),
            sender(mark_out, mark_in.at[me_s], mark_s.at[k], mark_r.at[k], peer),
            sender(edge_out, edge_in.at[me_s], edge_s.at[k], edge_r.at[k], peer),
        ]
    for copy in carry:
        copy.start()
    w_swaps = [
        sender(part.at[me_c], part.at[me_c], wp_s.at[k], wp_r.at[k], partner)
        for k, part in enumerate((w_gate, w_up, w_down))
    ]
    carry_in[pl.ds(me_s, 1)] = carry_out[...][None]
    mark_in[pl.ds(me_s, 1)] = mark_out[...][None]
    edge_in[pl.ds(me_s, 1)] = edge_out[...][None]
    loads[6].wait()
    loads[7].wait()
    expert = lax.broadcasted_iota(jnp.int32, weights_ref.shape, 0)
    shares = jnp.zeros(weights_ref.shape, jnp.float32)
    for k in range(routes_ref.shape[0]):
        shares = shares + jnp.where(
            routes_ref[k : k + 1] == expert, route_w_ref[k : k + 1], 0.0
        )
    weights_ref[...] = shares
    share = [
        sender(weights_ref, share_in.at[me_s], share_s.at[k], share_r.at[k], peer)
        for k, peer in enumerate(sp_peers)
    ]
    for copy in share:
        copy.start()
    share_in[pl.ds(me_s, 1)] = shares[None]
    for k in (9, 10, 11):
        loads[k].wait()
    raw = gate_ref[...].astype(jnp.float32)
    gelu = 0.5 * raw * (1.0 + jnp.tanh(GELU_SCALE * (raw + 0.044715 * raw * raw * raw)))
    gelu = gelu * gain_ref[...]
    w_loads[0].wait()
    w_swaps[0].start()
    for copy in carry:
        copy.wait()
    xs, now, prior = [], [], []
    for place in range(n_sp):
        marks = mark_in[place]
        now.append(jnp.broadcast_to(marks[:, 0:1], (8, LANES)))
        if place == 0:
            prior.append(jnp.full((8, LANES), -1, jnp.int32))
        else:
            prior.append(jnp.broadcast_to(mark_in[place - 1][:, 1:2], (8, LANES)))
        xs.append(
            jnp.concatenate(
                [
                    edge_in[max(place - 1, 0)].astype(jnp.float32)[24:],
                    edge_in[place].astype(jnp.float32)[:8],
                ],
                axis=0,
            )
        )
    both = [jnp.concatenate([prior[p], now[p]], axis=0) for p in range(n_sp)]
    head_starts = jnp.concatenate([both[p][7:15] != now[p] for p in range(n_sp)], axis=0)
    in_tile = lax.broadcasted_iota(jnp.int32, (8 * n_sp, LANES), 0) % 8
    for group in range(channels // LANES):
        span = slice(group * LANES, (group + 1) * LANES)
        sums = []
        for place in range(n_sp):
            total = jnp.zeros((8, LANES), jnp.float32)
            for tap in range(reach + 1):
                first = 8 - reach + tap
                same = both[place][first : first + 8] == now[place]
                total = total + (
                    jnp.where(same, xs[place][first : first + 8, span], 0.0)
                    * taps[tap : tap + 1, span]
                )
            sums.append(total)
        step, state = gates(jnp.concatenate(sums, axis=0).astype(jnp.bfloat16), head_starts, group)
        for distance in (1, 2, 4):
            inside = in_tile >= distance
            state = state + step * jnp.where(inside, pltpu.roll(state, distance, 0), 0.0)
            step = step * jnp.where(inside, pltpu.roll(step, distance, 0), 1.0)
        head_a[:, :, span] = step.reshape(n_sp, 8, LANES)
        head_b[:, :, span] = state.reshape(n_sp, 8, LANES)
    carried = jnp.zeros((1, channels), jnp.float32)
    for place in range(n_sp - 1):
        entered = head_b[place][7:] + head_a[place][7:] * carried
        tile = carry_in[place]
        carried = jnp.where(place < me_s, tile[1:2] + tile[0:1] * entered, carried)
    top = head_b[pl.ds(me_s, 1)][0] + head_a[pl.ds(me_s, 1)][0] * carried
    hidden = jnp.concatenate([top, run_b[8:] + run_a[8:] * top[7:]], axis=0)
    row_squares = jnp.sum(hidden * hidden, axis=1, keepdims=True)
    for place in range(n_tp):
        packed = jnp.zeros((8, LANES), jnp.float32)
        for j in range(piece // 8):
            first = place * piece + j * 8
            packed = jnp.where(lane8 == j, row_squares[first : first + 8], packed)
        squares[place] = packed
    loads[LATE].wait()
    mixer = (hidden * gelu).astype(jnp.bfloat16)
    tile_width = min(512, width)
    for first in range(0, width, tile_width):
        span = slice(first, first + tile_width)
        product = jnp.dot(mixer, out_w_ref[:, span], preferred_element_type=jnp.float32)
        parts[:, :, span] = product.astype(jnp.bfloat16).reshape(n_tp, piece, tile_width)

    half = width // 2
    halves = (pl.ds(0, half), pl.ds(half, half))
    pair = []
    for i in (3, 2, 1, 0):
        theirs = across[i] * 2 + 1 - me_c
        pair.append(
            (
                sender(squares.at[theirs], square_pair.at[i], pair_s.at[1, i], pair_r.at[1, i], partner),
                sender(parts.at[theirs], pair_in.at[i], pair_s.at[0, i], pair_r.at[0, i], partner),
            )
        )
        for copy in pair[-1]:
            copy.start()
    square_copies = []
    inward = {}
    for i in (3, 2, 1):
        for h in range(2):
            inward[i, h] = sender(
                z_out.at[i, :, halves[h]], z_in.at[i, :, halves[h]], z_s.at[h, i], z_r.at[h, i], near
            )
    for n, i in enumerate((3, 2, 1, 0)):
        mine = across[i] * 2 + me_c
        for copy in pair[n]:
            copy.wait_recv()
        square_out[i] = squares[mine] + square_pair[i]
        if i > 0:
            copy = sender(
                square_out.at[i], square_in.at[me_z], sq_s.at[i], sq_r.at[me_z], z_peers[i - 1]
            )
            copy.start()
            square_copies.append(copy)
        z_out[i] = (
            parts[mine].astype(jnp.float32) + pair_in[i].astype(jnp.float32)
        ).astype(jnp.bfloat16)

        if i > 0:

            @pl.when(outer)
            def _():
                for h in range(2):
                    inward[i, h].start()

    for k in (1, 2):
        w_loads[k].wait()
        w_swaps[k].start()
    crossing, outward = {}, {}
    for i in (3, 2):
        for h in range(2):
            crossing[i, h] = sender(
                z_sum.at[i, :, halves[h]], z_across.at[i, :, halves[h]], z_s.at[h, i + 2], z_r.at[h, i + 2], over
            )
    for h in range(2):
        outward[h] = sender(
            z_sum.at[1, :, halves[h]], z_in.at[0, :, halves[h]], z_s.at[h, 0], z_r.at[h, 0], near
        )

    @pl.when(middle)
    def _():
        def add_up(target, i, h, received):
            span = slice(h * half, (h + 1) * half)
            target[i, :, span] = (
                z_out[i, :, span].astype(jnp.float32) + received[:, span].astype(jnp.float32)
            ).astype(jnp.bfloat16)

        for i, h in ((3, 0), (3, 1), (2, 0)):
            inward[i, h].wait_recv()
            add_up(z_sum, i, h, z_in.at[i])
            crossing[i, h].start()
        for h in range(2):
            if h == 1:
                inward[2, 1].wait_recv()
                add_up(z_sum, 2, 1, z_in.at[2])
                crossing[2, 1].start()
            crossing[3, h].wait_recv()
            add_up(z_sum, 1, h, z_across.at[3])
            outward[h].start()
        for h in range(2):
            inward[1, h].wait_recv()
            add_up(z_sum, 0, h, z_in.at[1])
        for h in range(2):
            crossing[2, h].wait_recv()
        z_in[0] = (z_sum[0].astype(jnp.float32) + z_across[2].astype(jnp.float32)).astype(jnp.bfloat16)
        z_sum[0] = z_in[0]

    @pl.when(outer)
    def _():
        for h in range(2):
            outward[h].wait_recv()
        z_sum[0] = (z_out[0].astype(jnp.float32) + z_in[0].astype(jnp.float32)).astype(jnp.bfloat16)

    summed = z_sum[0].astype(jnp.float32)
    square_sum = square_out[0]
    for k in range(1, n_z):
        from_z = (me_z + k) % n_z
        sender(
            square_out.at[0], square_in.at[from_z], sq_s.at[0], sq_r.at[from_z], near
        ).wait_recv()
        square_sum = square_sum + square_in[pl.ds(from_z, 1)][0]
    square_sum = jnp.concatenate(
        [square_sum[:, j : j + 1] for j in range(piece // 8)], axis=0
    )
    inverse = lax.rsqrt(square_sum / (channels * n_tp) + EPSILON)
    residual_copy.wait()
    own = (res_rows[...].astype(jnp.float32) + summed * inverse).astype(jnp.bfloat16)
    own_ref[...] = own
    floated = own.astype(jnp.float32)
    inverse = lax.rsqrt(jnp.mean(floated * floated, axis=1, keepdims=True) + EPSILON)
    normed_ref[...] = (floated * inverse * ffn_ref[...]).astype(jnp.bfloat16)

    lower, upper = halves
    sent = []

    def push(source, target, sems, slot, peer):
        copy = sender(source, target, sems[0].at[slot], sems[1].at[slot], peer)
        copy.start()
        sent.append(copy)
        return copy

    gz, gxy, gd = (gz_s, gz_r), (gxy_s, gxy_r), (gd_s, gd_r)
    r1, r2, rz = (r1_s, r1_r), (r2_s, r2_r), (rz_s, rz_r)
    from_x, from_y, from_da, from_db = {}, {}, {}, {}
    mid_sent = []

    def arrival(i, h):
        part = blocks.at[i, me_s, :, halves[h]]
        return sender(part, part, gz[0].at[h, i], gz[1].at[h, i], near)

    def mid_push(source, i, h, slot, peer):
        part = blocks.at[i, me_s, :, halves[h]]
        copy = sender(source.at[:, halves[h]], part, gz[0].at[h, slot], gz[1].at[h, i], peer)
        pl.when(middle)(copy.start)
        mid_sent.append(copy)

    def pass_on(i, h):
        pl.when(middle)(arrival(i, h).wait_recv)
        mid_push(blocks.at[i, me_s], i, h, i + 2, near)

    def spread(i):
        block = blocks.at[i, me_s]
        source = normed_ref if i == 0 else block

        def ready(h):
            if i == 1:
                arrival(1, h).wait_recv()
                mid_push(source, 3, h, 3, over)
            elif i > 1:
                pl.when(outer)(arrival(i, h).wait_recv)

        def to_x(h):
            part = halves[h]
            from_x[h, i] = push(source.at[:, part], block.at[:, part], gxy, (h, i), x_peer)

        def to_y(h):
            part = halves[h]
            from_y[h, i] = push(source.at[:, part], block.at[:, part], gxy, (2 + h, i), y_peer)

        ready(0)
        to_x(0)
        ready(1)
        to_y(1)
        to_x(1)
        to_y(0)
        if i == 0:
            for h in range(2):
                part = halves[h]
                sent.append(
                    sender(
                        source.at[:, part],
                        blocks.at[1, me_s, :, part],
                        gz[0].at[h, 1],
                        gz[1].at[h, 1],
                        near,
                    )
                )
                sent[-1].start()
                mid_push(source, 2, h, 2, over)

    def relay(i):
        from_x[0, i].wait_recv()
        part = blocks.at[i, s_x, :, lower]
        from_da[i] = push(part, part, gd, (0, i), y_peer)
        from_y[1, i].wait_recv()
        part = blocks.at[i, s_y, :, upper]
        from_db[i] = push(part, part, gd, (1, i), x_peer)

    def gathered(i):
        from_x[1, i].wait_recv()
        from_y[0, i].wait_recv()
        from_da[i].wait_recv()
        from_db[i].wait_recv()

    own_copy = pltpu.make_async_copy(normed_ref, blocks.at[0, me_s], own_sem)
    own_copy.start()
    spread(0)
    for copy in share:
        copy.wait()
    for place in range(n_sp):
        turned = jnp.transpose(share_in[place])
        lane = lax.broadcasted_iota(jnp.int32, turned.shape, 1)
        chosen = jnp.sum(jnp.where(lane == me_s, turned, 0.0), axis=1, keepdims=True)
        share_cols[place] = jnp.broadcast_to(chosen, (rows, LANES))

    ff = w_gate.shape[2]
    f_tile, d_tile = 256, min(512, width)
    count = n_sp * piece
    first_xs, first_ys, second_xs, second_ys = {}, {}, {}, {}
    slabs = ff // f_tile

    def swapped(k):
        w_swaps[k].wait_recv()

    def rise(i, step):
        tokens = blocks[i].reshape(count, width)
        for tile in (2 * step, 2 * step + 1):
            core, span = tile // slabs, pl.ds(tile % slabs * f_tile, f_tile)
            gate_part = jnp.dot(tokens, w_gate[core, :, span], preferred_element_type=jnp.float32)
            up_part = jnp.dot(tokens, w_up[core, :, span], preferred_element_type=jnp.float32)
            hidden_units[:, tile * f_tile : (tile + 1) * f_tile] = (
                gate_part * jax.nn.sigmoid(gate_part) * up_part
            ).astype(jnp.bfloat16)

    def fall(i, h):
        first = pl.multiple_of(across[i] * (2 * piece) + me_c * piece, piece)
        scale = share_cols[:, pl.ds(first, piece), :].reshape(count, LANES)[:, :1]
        units = hidden_units[...]
        for step in range(half // d_tile):
            begin = h * half + step * d_tile
            span = slice(begin, begin + d_tile)
            product = jnp.dot(
                units,
                w_down[:, :, span].reshape(2 * ff, d_tile),
                preferred_element_type=jnp.float32,
            )
            joined[i, :, :, span] = (
                (product * scale).astype(jnp.bfloat16).reshape(n_sp, piece, d_tile)
            )

    def depart(i, h):
        if h == 0:
            first_xs[1, i] = push(joined.at[i, s_d, :, lower], first_x.at[1, i], r1, (2, i), x_peer)
            first_xs[0, i] = push(joined.at[i, s_x, :, lower], first_x.at[0, i], r1, (0, i), x_peer)
        else:
            first_ys[1, i] = push(joined.at[i, s_d, :, upper], first_y.at[1, i], r1, (3, i), y_peer)
            first_ys[0, i] = push(joined.at[i, s_y, :, upper], first_y.at[0, i], r1, (1, i), y_peer)

    def turn(i):
        first_xs[1, i].wait_recv()
        relay_a[i] = (
            joined[i, s_y, :, :half].astype(jnp.float32) + first_x[1, i].astype(jnp.float32)
        ).astype(jnp.bfloat16)
        second_ys[i] = push(relay_a.at[i], second_y.at[i], r2, (0, i), y_peer)
        first_ys[1, i].wait_recv()
        relay_b[i] = (
            joined[i, s_x, :, half:].astype(jnp.float32) + first_y[1, i].astype(jnp.float32)
        ).astype(jnp.bfloat16)
        second_xs[i] = push(relay_b.at[i], second_x.at[i], r2, (1, i), x_peer)

    def finish(i):
        for copies in (first_xs, first_ys):
            copies[0, i].wait_recv()
        for copies in (second_xs, second_ys):
            copies[i].wait_recv()
        low = (
            joined[i, me_s, :, :half].astype(jnp.float32)
            + first_x[0, i].astype(jnp.float32)
            + second_y[i].astype(jnp.float32)
        )
        high = (
            joined[i, me_s, :, half:].astype(jnp.float32)
            + first_y[0, i].astype(jnp.float32)
            + second_x[i].astype(jnp.float32)
        )
        column[i] = jnp.concatenate([low, high], axis=1).astype(jnp.bfloat16)
        if i in (1, 3):
            copy = sender(
                column.at[i], last_in.at[me_z], rz[0].at[0, i], rz[1].at[0, me_z], z_peers[i - 1]
            )
            copy.start()
            sent.append(copy)
        elif i == 2:
            for h in range(2):
                pl.when(outer)(homeward[h].start)

    homeward, crossed = [], []
    for h in range(2):
        part = halves[h]
        homeward.append(
            sender(
                column.at[2, :, part],
                last_in.at[z_near, :, part],
                rz[0].at[h, 2],
                rz[1].at[h, z_near],
                near,
            )
        )
        crossed.append(
            sender(
                relay_c.at[:, part],
                last_in.at[me_z, :, part],
                rz[0].at[h, 2],
                rz[1].at[h, me_z],
                over,
            )
        )

    def cross(i):
        @pl.when(middle)
        def _():
            for h in range(2):
                span = slice(h * half, (h + 1) * half)
                part = last_in.at[me_z, :, halves[h]]
                sender(part, part, rz[0].at[h, 2], rz[1].at[h, me_z], near).wait_recv()
                relay_c[:, span] = (
                    column[i, :, span].astype(jnp.float32)
                    + last_in[me_z, :, span].astype(jnp.float32)
                ).astype(jnp.bfloat16)
                crossed[h].start()

    own_copy.wait()
    plan = (
        (relay, 0),
        (pass_on, 2, 0),
        (pass_on, 2, 1),
        (spread, 1),
        (gathered, 0),
        (swapped, 0),
        (swapped, 1),
        (rise, 0, 0),
        (relay, 1),
        (rise, 0, 1),
        (spread, 2),
        (pass_on, 3, 0),
        (pass_on, 3, 1),
        (rise, 0, 2),
        (swapped, 2),
        (fall, 0, 0),
        (fall, 0, 1),
        (gathered, 1),
        (rise, 1, 0),
        (relay, 2),
        (rise, 1, 1),
        (spread, 3),
        (rise, 1, 2),
        (fall, 1, 0),
        (fall, 1, 1),
        (gathered, 2),
        (rise, 2, 0),
        (rise, 2, 1),
        (relay, 3),
        (depart, 1, 0),
        (depart, 1, 1),
        (rise, 2, 2),
        (fall, 2, 0),
        (depart, 2, 0),
        (fall, 2, 1),
        (depart, 2, 1),
        (gathered, 3),
        (rise, 3, 0),
        (turn, 1),
        (rise, 3, 1),
        (rise, 3, 2),
        (fall, 3, 0),
        (depart, 3, 0),
        (fall, 3, 1),
        (depart, 3, 1),
        (turn, 2),
        (finish, 1),
        (turn, 3),
        (depart, 0, 0),
        (depart, 0, 1),
        (finish, 2),
        (finish, 3),
        (turn, 0),
        (cross, 2),
        (finish, 0),
    )
    for stage, *at in plan:
        stage(*at)
    total = own_ref[...].astype(jnp.float32) + column[0].astype(jnp.float32)
    def landed(h, z):
        if h is None:
            sender(column.at[0], last_in.at[z], rz[0].at[0, 0], rz[1].at[0, z], near).wait_recv()
        else:
            part = last_in.at[z, :, halves[h]]
            sender(part, part, rz[0].at[h, 0], rz[1].at[h, z], near).wait_recv()

    landed(None, z_near)
    total = total + last_in[z_near].astype(jnp.float32)

    @pl.when(outer)
    def _():
        landed(None, across[2])
        landed(None, z_far)

    @pl.when(middle)
    def _():
        landed(0, z_far)
        landed(1, z_far)
        last_in[me_z] = jnp.zeros(last_in.shape[1:], last_in.dtype)

    total = total + last_in[z_far].astype(jnp.float32)
    last = jnp.where(middle, me_z, across[2])
    total = total + last_in[pl.ds(last, 1)][0].astype(jnp.float32)
    out_ref[...] = total.astype(jnp.bfloat16)
    for copies in pair:
        for copy in copies:
            copy.wait_send()
    for copy in square_copies + w_swaps:
        copy.wait_send()

    @pl.when(outer)
    def _():
        for copy in list(inward.values()) + homeward:
            copy.wait_send()

    @pl.when(middle)
    def _():
        for copy in list(crossing.values()) + list(outward.values()) + mid_sent + crossed:
            copy.wait_send()

    for copy in sent:
        copy.wait_send()


def dense_local(
    lru_input,
    gate_input,
    documents,
    conv_taps,
    rate_weight,
    inlet_weight,
    decay_param,
    lru_gain,
    out_weight,
    residual,
    ffn_gain,
    routes,
    route_weights,
    w_gate,
    w_up,
    w_down,
):
    n_sp, n_tp = lax.axis_size("sp"), lax.axis_size("tp")
    n_z = n_tp // 2
    rows, channels = lru_input.shape
    width = residual.shape[1]
    ff = w_gate.shape[2]
    piece = rows // n_tp
    padded = -(-n_sp // 8) * 8
    vmem = pl.BlockSpec(memory_space=pltpu.VMEM)
    half = width // 2
    top = routes.shape[1]
    hbm = pl.BlockSpec(memory_space=pl.ANY)
    bf16, f32 = jnp.bfloat16, jnp.float32
    dma = pltpu.SemaphoreType.DMA
    rows_buffer = pltpu.VMEM((n_z, piece, width), bf16)
    half_buffer = pltpu.VMEM((n_z, piece, half), bf16)
    groups = pltpu.VMEM((n_z, n_sp, piece, width), bf16)
    square_buffer = pltpu.VMEM((n_z, 8, LANES), f32)
    shapes = (
        [(n_sp,)] * 8
        + [(2, n_z)] * 2
        + [(2, n_z + 2)] * 2
        + [(n_z,)] * 2
        + [(2, n_z + 2)] * 2
        + [(4, n_z)] * 2
        + [(2, n_z)] * 2
        + [(3,)] * 2
        + [(4, n_z)] * 2
        + [(2, n_z)] * 2
        + [(2, n_z)] * 2
    )
    return pl.pallas_call(
        functools.partial(layer_kernel, n_sp, n_tp),
        out_shape=jax.ShapeDtypeStruct((piece, width), bf16),
        in_specs=[hbm] * 16,
        out_specs=vmem,
        scratch_shapes=[
            pltpu.VMEM((rows, channels), bf16),
            pltpu.VMEM((rows, channels), bf16),
            pltpu.VMEM((1, rows), jnp.int32),
            pltpu.VMEM(conv_taps.shape, bf16),
            pltpu.VMEM(rate_weight.shape, bf16),
            pltpu.VMEM(inlet_weight.shape, bf16),
            pltpu.VMEM((1, channels), f32),
            pltpu.VMEM((1, channels), f32),
            pltpu.VMEM((channels, width), bf16),
            pltpu.VMEM((1, width), f32),
            pltpu.VMEM((top, rows), jnp.int32),
            pltpu.VMEM((top, rows), f32),
            pltpu.VMEM((rows, LANES), jnp.int32),
            pltpu.VMEM((padded, rows), f32),
            pltpu.VMEM((32, channels), bf16),
            pltpu.VMEM((n_sp, 32, channels), bf16),
            pltpu.VMEM((8, LANES), jnp.int32),
            pltpu.VMEM((n_sp, 8, LANES), jnp.int32),
            pltpu.VMEM((8, channels), f32),
            pltpu.VMEM((n_sp, 8, channels), f32),
            pltpu.VMEM((n_sp, 8, channels), f32),
            pltpu.VMEM((n_sp, 8, channels), f32),
            pltpu.VMEM((n_sp, padded, rows), f32),
            pltpu.VMEM((rows, channels), f32),
            pltpu.VMEM((rows, channels), f32),
            pltpu.VMEM((n_tp, piece, width), bf16),
            rows_buffer,
            rows_buffer,
            rows_buffer,
            rows_buffer,
            rows_buffer,
            pltpu.VMEM((n_tp, 8, LANES), f32),
            square_buffer,
            square_buffer,
            square_buffer,
            pltpu.VMEM((piece, width), bf16),
            pltpu.VMEM((piece, width), bf16),
            pltpu.VMEM((piece, width), bf16),
            pltpu.VMEM((2, width, ff), bf16),
            pltpu.VMEM((2, width, ff), bf16),
            pltpu.VMEM((2, ff, width), bf16),
            pltpu.VMEM((n_sp, rows, LANES), f32),
            groups,
            pltpu.VMEM((n_sp * piece, 2 * ff), bf16),
            groups,
            pltpu.VMEM((2, n_z, piece, half), bf16),
            pltpu.VMEM((2, n_z, piece, half), bf16),
            half_buffer,
            half_buffer,
            half_buffer,
            half_buffer,
            pltpu.VMEM((piece, width), bf16),
            rows_buffer,
            rows_buffer,
            dma((12,)),
            dma,
            dma((3,)),
            dma,
        ]
        + [dma(shape) for shape in shapes],
        compiler_params=pltpu.CompilerParams(
            collective_id=0, has_side_effects=True, vmem_limit_bytes=60 * 2**20
        ),
    )(
        lru_input,
        gate_input,
        documents[None, :],
        conv_taps,
        rate_weight,
        inlet_weight,
        decay_param[None, :],
        lru_gain[None, :],
        out_weight,
        residual,
        ffn_gain[None, :],
        routes.T,
        route_weights.T,
        w_gate[0],
        w_up[0],
        w_down[0],
    )


def solution(mesh):
    n_sp, n_tp = mesh.shape["sp"], mesh.shape["tp"]
    body = dense_local if n_sp == 4 and n_tp == 8 else local
    return jax.shard_map(
        body,
        mesh=mesh,
        in_specs=(
            P("sp", "tp"),
            P("sp", "tp"),
            P("sp"),
            P(None, "tp"),
            P("tp", None, None),
            P("tp", None, None),
            P("tp"),
            P("tp"),
            P("tp", None),
            P("sp", None),
            P(),
            P("sp", None),
            P("sp", None),
            P("sp", None, "tp"),
            P("sp", None, "tp"),
            P("sp", "tp", None),
        ),
        out_specs=P(("sp", "tp"), None),
        check_vma=False,
    )
```

```python
import functools

import jax
import jax.numpy as jnp
from jax import lax
from jax.experimental import pallas as pl
from jax.experimental.pallas import tpu as pltpu
from jax.sharding import PartitionSpec as P

D_RNN = 2048


EPSILON = 1e-06
RATE_SCALE = 8.0


def shifted(block, axis, distance):
    devices = range(lax.axis_size(axis))
    route = [(i - distance, i) for i in devices if i - distance in devices]
    return lax.ppermute(block, axis, route)


def carried_in(value, axis, join, neutral):
    count, mine = (lax.axis_size(axis), lax.axis_index(axis))
    pieces = jax.tree.map(lambda part: lax.all_gather(part, axis), value)
    so_far = jax.tree.map(
        lambda part, zero: jnp.full_like(part, 0) + jnp.asarray(zero, part.dtype), value, neutral
    )

    def hop(position, so_far):
        longer = join(so_far, jax.tree.map(lambda part: part[position], pieces))
        return jax.tree.map(lambda new, old: jnp.where(position < mine, new, old), longer, so_far)

    return lax.fori_loop(0, count - 1, hop, so_far)


def join_runs(earlier_run, later_run):
    return (earlier_run[0] * later_run[0], later_run[0] * earlier_run[1] + later_run[1])


def slot_targets(route_block, expert_count, capacity):
    flat_routes = route_block.reshape(-1)
    onehot = (flat_routes[:, None] == jnp.arange(expert_count, dtype=jnp.int32)[None, :]).astype(
        jnp.int32
    )
    earlier_hits = jnp.cumsum(onehot, axis=0) - onehot
    slot_index = jnp.sum(earlier_hits * onehot, axis=1)
    return (flat_routes * capacity + slot_index).reshape(route_block.shape)


def pick_matrix(targets, slot_total):
    slot_hits = targets[None, :, :] == jnp.arange(slot_total, dtype=jnp.int32)[:, None, None]
    return jnp.sum(slot_hits.astype(jnp.int32), axis=2).astype(jnp.bfloat16)


def rms_rows(row_block, gain_vector):
    floated = row_block.astype(jnp.float32)
    inverse_rms = lax.rsqrt(jnp.mean(floated * floated, axis=1, keepdims=True) + EPSILON)
    return (floated * inverse_rms * gain_vector[None, :]).astype(jnp.bfloat16)


def expert_apply(row_piece, gate_weight, up_weight, down_weight):
    gate_part = jnp.dot(row_piece, gate_weight, preferred_element_type=jnp.float32)
    up_part = jnp.dot(row_piece, up_weight, preferred_element_type=jnp.float32)
    hidden_units = (jax.nn.silu(gate_part) * up_part).astype(jnp.bfloat16)
    return jnp.dot(hidden_units, down_weight, preferred_element_type=jnp.float32)


def local(
    lru_input,
    gate_input,
    documents,
    conv_taps,
    rate_weight,
    inlet_weight,
    decay_param,
    lru_gain,
    out_weight,
    residual,
    ffn_gain,
    routes,
    route_weights,
    w_gate,
    w_up,
    w_down,
):
    positions = lru_input.shape[0]
    channels = lru_input.shape[1]
    model_width = residual.shape[1]
    reach_back = conv_taps.shape[0] - 1
    tail_rows, tail_docs = shifted(
        (lru_input[positions - reach_back :], documents[positions - reach_back :] + 1), "sp", 1
    )
    prior_docs = jnp.concatenate([tail_docs - 1, documents])
    padded_input = jnp.concatenate([tail_rows, lru_input], axis=0)
    conv_sum = jnp.zeros((positions, channels), jnp.float32)
    for tap_index in range(reach_back + 1):
        same_doc = (prior_docs[tap_index : tap_index + positions] == documents).astype(jnp.float32)[
            :, None
        ]
        conv_sum = (
            conv_sum
            + padded_input[tap_index : tap_index + positions].astype(jnp.float32)
            * conv_taps[tap_index].astype(jnp.float32)[None, :]
            * same_doc
        )
    convolved = conv_sum.astype(jnp.bfloat16)
    grouped = convolved.reshape(positions, rate_weight.shape[0], rate_weight.shape[1])
    rate_gate = jax.nn.sigmoid(
        jnp.einsum(
            "tnc,ncd->tnd", grouped, rate_weight, preferred_element_type=jnp.float32
        ).reshape(positions, channels)
    )
    inlet_gate = jax.nn.sigmoid(
        jnp.einsum(
            "tnc,ncd->tnd", grouped, inlet_weight, preferred_element_type=jnp.float32
        ).reshape(positions, channels)
    )
    log_decay = -RATE_SCALE * rate_gate * jax.nn.softplus(-decay_param)[None, :]
    starts = (prior_docs[reach_back - 1 : reach_back - 1 + positions] != documents)[:, None]
    decay_step = jnp.where(starts, 0.0, jnp.exp(log_decay))
    norm_factor = jnp.where(starts, 1.0, jnp.sqrt(-jnp.expm1(2.0 * log_decay)))
    drive_term = norm_factor * inlet_gate * convolved.astype(jnp.float32)
    decay_run, local_state = lax.associative_scan(join_runs, (decay_step, drive_term), axis=0)
    carried = carried_in(
        (decay_run[positions - 1], local_state[positions - 1]),
        "sp",
        join_runs,
        (jnp.ones((channels,), jnp.float32), jnp.zeros((channels,), jnp.float32)),
    )
    hidden_state = local_state + decay_run * carried[1][None, :]
    square_sums = lax.psum(jnp.sum(hidden_state * hidden_state, axis=1), "tp")
    inverse_rms = lax.rsqrt(square_sums[:, None] / D_RNN + EPSILON)
    mixer_rows = (
        hidden_state * inverse_rms * lru_gain[None, :] * jax.nn.gelu(gate_input.astype(jnp.float32))
    ).astype(jnp.bfloat16)
    tp_count = lax.axis_size("tp")
    tp_here = lax.axis_index("tp")
    expert_count = lax.axis_size("sp")
    route_rows = positions // tp_count
    top_count = routes.shape[1]
    capacity = 2 * top_count * route_rows // expert_count
    slot_total = expert_count * capacity
    projected = lax.psum_scatter(
        jnp.dot(mixer_rows, out_weight, preferred_element_type=jnp.float32).astype(jnp.bfloat16),
        "tp",
        scatter_dimension=0,
        tiled=True,
    ).astype(jnp.float32)
    own_rows = (
        lax.dynamic_slice_in_dim(residual, tp_here * route_rows, route_rows, 0).astype(jnp.float32)
        + projected
    ).astype(jnp.bfloat16)
    own_routes = lax.dynamic_slice_in_dim(routes, tp_here * route_rows, route_rows, 0)
    targets = slot_targets(own_routes, expert_count, capacity)
    outgoing = jnp.dot(
        pick_matrix(targets, slot_total),
        rms_rows(own_rows, ffn_gain),
        preferred_element_type=jnp.float32,
    ).astype(jnp.bfloat16)
    arrived = lax.all_to_all(
        outgoing.reshape(expert_count, capacity, model_width),
        "sp",
        split_axis=0,
        concat_axis=0,
        tiled=True,
    )
    partial_out = expert_apply(
        lax.all_gather(arrived.reshape(slot_total, model_width), "tp", axis=0, tiled=True),
        w_gate[0],
        w_up[0],
        w_down[0],
    )
    expert_out = lax.psum_scatter(
        partial_out.astype(jnp.bfloat16), "tp", scatter_dimension=0, tiled=True
    )
    returned = lax.all_to_all(
        expert_out.reshape(expert_count, capacity, model_width),
        "sp",
        split_axis=0,
        concat_axis=0,
        tiled=True,
    )
    picked = returned.reshape(slot_total, model_width)[targets.reshape(-1)].astype(jnp.float32)
    picked = picked.reshape(route_rows, top_count, model_width)
    own_weights = lax.dynamic_slice_in_dim(route_weights, tp_here * route_rows, route_rows, 0)
    routed = jnp.sum(picked * own_weights[:, :, None], axis=1)
    return (own_rows.astype(jnp.float32) + routed).astype(jnp.bfloat16)


MESH = pl.DeviceIdType.MESH
LANES = 128
GELU_SCALE = 0.7978845608028654


def sender(source, target, send_sem, recv_sem, peer):
    return pltpu.make_async_remote_copy(
        src_ref=source,
        dst_ref=target,
        send_sem=send_sem,
        recv_sem=recv_sem,
        device_id=peer,
        device_id_type=MESH,
    )


def greet(peers):
    barrier = pltpu.get_barrier_semaphore()
    for peer in peers:
        pl.semaphore_signal(barrier, inc=1, device_id=peer, device_id_type=MESH)
    pl.semaphore_wait(barrier, len(peers))


def one_minus_exp(value):
    series = 1.0 + value * (1.0 / 6.0)
    for order in (5.0, 4.0, 3.0, 2.0):
        series = 1.0 + value * (1.0 / order) * series
    return jnp.where(value > -0.25, -value * series, 1.0 - jnp.exp(value))


def down_by(block, distance, filler):
    count = block.shape[0]
    if distance % 8 == 0:
        top = jnp.full((distance, block.shape[1]), filler, block.dtype)
        return jnp.concatenate([top, block[: count - distance]], axis=0)
    row = lax.broadcasted_iota(jnp.int32, block.shape, 0)
    return jnp.where(row >= distance, pltpu.roll(block, distance, 0), filler)


LATE = 8


def layer_kernel(
    n_sp,
    n_tp,
    lru_hbm,
    gate_hbm,
    docs_hbm,
    taps_hbm,
    rate_hbm,
    inlet_hbm,
    decay_hbm,
    gain_hbm,
    out_w_hbm,
    residual_hbm,
    ffn_hbm,
    routes_hbm,
    shares_hbm,
    w_gate_hbm,
    w_up_hbm,
    w_down_hbm,
    out_ref,
    lru_ref,
    gate_ref,
    docs_row,
    taps_ref,
    rate_ref,
    inlet_ref,
    decay_ref,
    gain_ref,
    out_w_ref,
    ffn_ref,
    routes_ref,
    route_w_ref,
    docs_ref,
    weights_ref,
    edge_out,
    edge_in,
    mark_out,
    mark_in,
    carry_out,
    carry_in,
    head_a,
    head_b,
    share_in,
    run_a,
    run_b,
    parts,
    pair_in,
    z_out,
    z_in,
    z_sum,
    z_across,
    squares,
    square_pair,
    square_out,
    square_in,
    res_rows,
    own_ref,
    normed_ref,
    w_gate,
    w_up,
    w_down,
    share_cols,
    blocks,
    hidden_units,
    joined,
    first_x,
    first_y,
    second_x,
    second_y,
    relay_a,
    relay_b,
    relay_c,
    column,
    last_in,
    load_sem,
    res_sem,
    w_sem,
    own_sem,
    edge_s,
    edge_r,
    mark_s,
    mark_r,
    carry_s,
    carry_r,
    share_s,
    share_r,
    pair_s,
    pair_r,
    z_s,
    z_r,
    sq_s,
    sq_r,
    gz_s,
    gz_r,
    gxy_s,
    gxy_r,
    gd_s,
    gd_r,
    wp_s,
    wp_r,
    r1_s,
    r1_r,
    r2_s,
    r2_r,
    rz_s,
    rz_r,
):
    me_s, me_t = lax.axis_index("sp"), lax.axis_index("tp")
    n_z = n_tp // 2
    me_z, me_c = me_t // 2, me_t % 2
    rows, channels = lru_ref.shape
    width = out_w_ref.shape[1]
    piece = rows // n_tp
    pairs = (
        (lru_hbm, lru_ref),
        (docs_hbm, docs_row),
        (taps_hbm, taps_ref),
        (rate_hbm, rate_ref),
        (inlet_hbm, inlet_ref),
        (decay_hbm, decay_ref),
        (routes_hbm, routes_ref),
        (shares_hbm, route_w_ref),
        (out_w_hbm, out_w_ref),
        (gate_hbm, gate_ref),
        (gain_hbm, gain_ref),
        (ffn_hbm, ffn_ref),
    )
    loads = [
        pltpu.make_async_copy(source, target, load_sem.at[k])
        for k, (source, target) in enumerate(pairs)
    ]
    for copy in loads:
        copy.start()
    residual_copy = pltpu.make_async_copy(
        residual_hbm.at[pl.ds(pl.multiple_of(me_t * piece, piece), piece)], res_rows, res_sem
    )
    residual_copy.start()
    w_loads = [
        pltpu.make_async_copy(source, target, w_sem.at[k])
        for k, (source, target) in enumerate(
            (
                (w_gate_hbm, w_gate.at[me_c]),
                (w_up_hbm, w_up.at[me_c]),
                (w_down_hbm, w_down.at[me_c]),
            )
        )
    ]
    s_x = me_s + 1 - 2 * (me_s % 2)
    s_y = (me_s + 2) % n_sp
    s_d = n_sp - 1 - me_s
    x_peer, y_peer = (s_x, me_t), (s_y, me_t)
    partner = (me_s, me_z * 2 + 1 - me_c)
    sp_peers = [((me_s + k) % n_sp, me_t) for k in range(1, n_sp)]
    z_near, z_far = me_z + 1 - 2 * (me_z % 2), n_z - 1 - me_z
    upper_side = me_z // 2
    across = (me_z, z_near, 2 - upper_side, 3 - 3 * upper_side)
    middle = (me_z + 1) // 2 % 2 == 1
    outer = (me_z + 1) // 2 % 2 == 0
    near, over = (me_s, z_near * 2 + me_c), (me_s, z_far * 2 + me_c)
    z_peers = [(me_s, across[k] * 2 + me_c) for k in range(1, n_z)]
    greeted = sp_peers + z_peers + [partner]
    barrier = pltpu.get_barrier_semaphore()
    for peer in greeted:
        pl.semaphore_signal(barrier, inc=1, device_id=peer, device_id_type=MESH)
    for k in range(6):
        loads[k].wait()
    for copy in w_loads:
        copy.start()
    docs = jnp.transpose(jnp.broadcast_to(docs_row[...], (8, rows)))
    docs = jnp.broadcast_to(docs[:, :1], (rows, LANES))
    docs_ref[...] = docs
    lane8 = lax.broadcasted_iota(jnp.int32, (8, LANES), 1)
    mark_out[...] = jnp.where(lane8 == 0, docs[:8], docs[rows - 8 :])
    edge_out[0:8] = lru_ref[0:8]
    edge_out[8:16] = lru_ref[rows - 8 :]
    taps = taps_ref[...].astype(jnp.float32)
    reach = taps.shape[0] - 1

    def gates(convolved, starts, group):
        span = slice(group * LANES, (group + 1) * LANES)
        rate = jax.nn.sigmoid(
            jnp.dot(convolved, rate_ref[group], preferred_element_type=jnp.float32)
        )
        inlet = jax.nn.sigmoid(
            jnp.dot(convolved, inlet_ref[group], preferred_element_type=jnp.float32)
        )
        minus = -decay_ref[:, span]
        soft = jnp.maximum(minus, 0.0) + jnp.log1p(jnp.exp(-jnp.abs(minus)))
        log_decay = -RATE_SCALE * rate * soft
        step = jnp.where(starts, 0.0, jnp.exp(log_decay))
        factor = jnp.where(starts, 1.0, jnp.sqrt(one_minus_exp(2.0 * log_decay)))
        return step, factor * inlet * convolved.astype(jnp.float32)

    body = rows - 8
    starts = docs[7 : 7 + body] != docs[8:]
    for group in range(channels // LANES):
        span = slice(group * LANES, (group + 1) * LANES)
        long = lru_ref[:, span].astype(jnp.float32)
        total = jnp.zeros((body, LANES), jnp.float32)
        for tap in range(reach + 1):
            first = 8 - reach + tap
            same = docs[first : first + body] == docs[8:]
            total = total + jnp.where(same, long[first : first + body], 0.0) * taps[tap : tap + 1, span]
        step, state = gates(total.astype(jnp.bfloat16), starts, group)
        distance = 1
        while distance < body:
            state = state + step * down_by(state, distance, 0.0)
            step = step * down_by(step, distance, 1.0)
            distance *= 2
        run_a[8:, span] = step
        run_b[8:, span] = state
        carry_out[:, span] = jnp.concatenate(
            [step[body - 1 :], state[body - 1 :], jnp.zeros((6, LANES), jnp.float32)], axis=0
        )
    pl.semaphore_wait(barrier, len(greeted))
    carry = []
    for k, peer in enumerate(sp_peers):
        carry += [
            sender(carry_out, carry_in.at[me_s], carry_s.at[k], carry_r.at[k], peer),
            sender(mark_out, mark_in.at[me_s], mark_s.at[k], mark_r.at[k], peer),
            sender(edge_out, edge_in.at[me_s], edge_s.at[k], edge_r.at[k], peer),
        ]
    for copy in carry:
        copy.start()
    w_swaps = [
        sender(part.at[me_c], part.at[me_c], wp_s.at[k], wp_r.at[k], partner)
        for k, part in enumerate((w_gate, w_up, w_down))
    ]
    carry_in[pl.ds(me_s, 1)] = carry_out[...][None]
    mark_in[pl.ds(me_s, 1)] = mark_out[...][None]
    edge_in[pl.ds(me_s, 1)] = edge_out[...][None]
    loads[6].wait()
    loads[7].wait()
    expert = lax.broadcasted_iota(jnp.int32, weights_ref.shape, 0)
    shares = jnp.zeros(weights_ref.shape, jnp.float32)
    for k in range(routes_ref.shape[0]):
        shares = shares + jnp.where(
            routes_ref[k : k + 1] == expert, route_w_ref[k : k + 1], 0.0
        )
    weights_ref[...] = shares
    share = [
        sender(weights_ref, share_in.at[me_s], share_s.at[k], share_r.at[k], peer)
        for k, peer in enumerate(sp_peers)
    ]
    for copy in share:
        copy.start()
    share_in[pl.ds(me_s, 1)] = shares[None]
    for k in (9, 10, 11):
        loads[k].wait()
    raw = gate_ref[...].astype(jnp.float32)
    gelu = 0.5 * raw * (1.0 + jnp.tanh(GELU_SCALE * (raw + 0.044715 * raw * raw * raw)))
    gelu = gelu * gain_ref[...]
    for copy in carry:
        copy.wait()
    xs, now, prior = [], [], []
    for place in range(n_sp):
        marks = mark_in[place]
        now.append(jnp.broadcast_to(marks[:, 0:1], (8, LANES)))
        if place == 0:
            prior.append(jnp.full((8, LANES), -1, jnp.int32))
        else:
            prior.append(jnp.broadcast_to(mark_in[place - 1][:, 1:2], (8, LANES)))
        xs.append(
            jnp.concatenate(
                [
                    edge_in[max(place - 1, 0)].astype(jnp.float32)[8:],
                    edge_in[place].astype(jnp.float32)[:8],
                ],
                axis=0,
            )
        )
    both = [jnp.concatenate([prior[p], now[p]], axis=0) for p in range(n_sp)]
    head_starts = jnp.concatenate([both[p][7:15] != now[p] for p in range(n_sp)], axis=0)
    in_tile = lax.broadcasted_iota(jnp.int32, (8 * n_sp, LANES), 0) % 8
    for group in range(channels // LANES):
        span = slice(group * LANES, (group + 1) * LANES)
        sums = []
        for place in range(n_sp):
            total = jnp.zeros((8, LANES), jnp.float32)
            for tap in range(reach + 1):
                first = 8 - reach + tap
                same = both[place][first : first + 8] == now[place]
                total = total + (
                    jnp.where(same, xs[place][first : first + 8, span], 0.0)
                    * taps[tap : tap + 1, span]
                )
            sums.append(total)
        step, state = gates(jnp.concatenate(sums, axis=0).astype(jnp.bfloat16), head_starts, group)
        for distance in (1, 2, 4):
            inside = in_tile >= distance
            state = state + step * jnp.where(inside, pltpu.roll(state, distance, 0), 0.0)
            step = step * jnp.where(inside, pltpu.roll(step, distance, 0), 1.0)
        head_a[:, :, span] = step.reshape(n_sp, 8, LANES)
        head_b[:, :, span] = state.reshape(n_sp, 8, LANES)
    carried = jnp.zeros((1, channels), jnp.float32)
    for place in range(n_sp - 1):
        entered = head_b[place][7:] + head_a[place][7:] * carried
        tile = carry_in[place]
        carried = jnp.where(place < me_s, tile[1:2] + tile[0:1] * entered, carried)
    top = head_b[pl.ds(me_s, 1)][0] + head_a[pl.ds(me_s, 1)][0] * carried
    hidden = jnp.concatenate([top, run_b[8:] + run_a[8:] * top[7:]], axis=0)
    row_squares = jnp.sum(hidden * hidden, axis=1, keepdims=True)
    for place in range(n_tp):
        packed = jnp.zeros((8, LANES), jnp.float32)
        for j in range(piece // 8):
            first = place * piece + j * 8
            packed = jnp.where(lane8 == j, row_squares[first : first + 8], packed)
        squares[place] = packed
    loads[LATE].wait()
    mixer = (hidden * gelu).astype(jnp.bfloat16)
    tile_width = min(512, width)
    for first in range(0, width, tile_width):
        span = slice(first, first + tile_width)
        product = jnp.dot(mixer, out_w_ref[:, span], preferred_element_type=jnp.float32)
        parts[:, :, span] = product.astype(jnp.bfloat16).reshape(n_tp, piece, tile_width)

    half = width // 2
    halves = (pl.ds(0, half), pl.ds(half, half))
    pair = []
    for i in (3, 2, 1, 0):
        theirs = across[i] * 2 + 1 - me_c
        pair.append(
            (
                sender(squares.at[theirs], square_pair.at[i], pair_s.at[1, i], pair_r.at[1, i], partner),
                sender(parts.at[theirs], pair_in.at[i], pair_s.at[0, i], pair_r.at[0, i], partner),
            )
        )
        for copy in pair[-1]:
            copy.start()
    square_copies = []
    inward = {}
    for i in (3, 2, 1):
        for h in range(2):
            inward[i, h] = sender(
                z_out.at[i, :, halves[h]], z_in.at[i, :, halves[h]], z_s.at[h, i], z_r.at[h, i], near
            )
    for n, i in enumerate((3, 2, 1, 0)):
        mine = across[i] * 2 + me_c
        for copy in pair[n]:
            copy.wait_recv()
        square_out[i] = squares[mine] + square_pair[i]
        if i > 0:
            copy = sender(
                square_out.at[i], square_in.at[me_z], sq_s.at[i], sq_r.at[me_z], z_peers[i - 1]
            )
            copy.start()
            square_copies.append(copy)
        z_out[i] = (
            parts[mine].astype(jnp.float32) + pair_in[i].astype(jnp.float32)
        ).astype(jnp.bfloat16)

        if i > 0:

            @pl.when(outer)
            def _():
                for h in range(2):
                    inward[i, h].start()

    for k in range(3):
        w_loads[k].wait()
        w_swaps[k].start()
    crossing, outward = {}, {}
    for i in (3, 2):
        for h in range(2):
            crossing[i, h] = sender(
                z_sum.at[i, :, halves[h]], z_across.at[i, :, halves[h]], z_s.at[h, i + 2], z_r.at[h, i + 2], over
            )
    for h in range(2):
        outward[h] = sender(
            z_sum.at[1, :, halves[h]], z_in.at[0, :, halves[h]], z_s.at[h, 0], z_r.at[h, 0], near
        )

    @pl.when(middle)
    def _():
        def add_up(target, i, h, received):
            span = slice(h * half, (h + 1) * half)
            target[i, :, span] = (
                z_out[i, :, span].astype(jnp.float32) + received[:, span].astype(jnp.float32)
            ).astype(jnp.bfloat16)

        for i, h in ((3, 0), (3, 1), (2, 0)):
            inward[i, h].wait_recv()
            add_up(z_sum, i, h, z_in.at[i])
            crossing[i, h].start()
        for h in range(2):
            if h == 1:
                inward[2, 1].wait_recv()
                add_up(z_sum, 2, 1, z_in.at[2])
                crossing[2, 1].start()
            crossing[3, h].wait_recv()
            add_up(z_sum, 1, h, z_across.at[3])
            outward[h].start()
        for h in range(2):
            inward[1, h].wait_recv()
            add_up(z_sum, 0, h, z_in.at[1])
        for h in range(2):
            crossing[2, h].wait_recv()
        z_in[0] = (z_sum[0].astype(jnp.float32) + z_across[2].astype(jnp.float32)).astype(jnp.bfloat16)
        z_sum[0] = z_in[0]

    @pl.when(outer)
    def _():
        for h in range(2):
            outward[h].wait_recv()
        z_sum[0] = (z_out[0].astype(jnp.float32) + z_in[0].astype(jnp.float32)).astype(jnp.bfloat16)

    summed = z_sum[0].astype(jnp.float32)
    square_sum = square_out[0]
    for k in range(1, n_z):
        from_z = (me_z + k) % n_z
        sender(
            square_out.at[0], square_in.at[from_z], sq_s.at[0], sq_r.at[from_z], near
        ).wait_recv()
        square_sum = square_sum + square_in[pl.ds(from_z, 1)][0]
    square_sum = jnp.concatenate(
        [square_sum[:, j : j + 1] for j in range(piece // 8)], axis=0
    )
    inverse = lax.rsqrt(square_sum / (channels * n_tp) + EPSILON)
    residual_copy.wait()
    own = (res_rows[...].astype(jnp.float32) + summed * inverse).astype(jnp.bfloat16)
    own_ref[...] = own
    floated = own.astype(jnp.float32)
    inverse = lax.rsqrt(jnp.mean(floated * floated, axis=1, keepdims=True) + EPSILON)
    normed_ref[...] = (floated * inverse * ffn_ref[...]).astype(jnp.bfloat16)

    lower, upper = halves
    sent = []

    def push(source, target, sems, slot, peer):
        copy = sender(source, target, sems[0].at[slot], sems[1].at[slot], peer)
        copy.start()
        sent.append(copy)
        return copy

    gz, gxy, gd = (gz_s, gz_r), (gxy_s, gxy_r), (gd_s, gd_r)
    r1, r2, rz = (r1_s, r1_r), (r2_s, r2_r), (rz_s, rz_r)
    from_x, from_y, from_da, from_db = {}, {}, {}, {}
    mid_sent = []

    def arrival(i, h):
        part = blocks.at[i, me_s, :, halves[h]]
        return sender(part, part, gz[0].at[h, i], gz[1].at[h, i], near)

    def mid_push(source, i, h, slot, peer):
        part = blocks.at[i, me_s, :, halves[h]]
        copy = sender(source.at[:, halves[h]], part, gz[0].at[h, slot], gz[1].at[h, i], peer)
        pl.when(middle)(copy.start)
        mid_sent.append(copy)

    def pass_on(i, h):
        pl.when(middle)(arrival(i, h).wait_recv)
        mid_push(blocks.at[i, me_s], i, h, i + 2, near)

    def spread(i):
        block = blocks.at[i, me_s]
        source = normed_ref if i == 0 else block

        def ready(h):
            if i == 1:
                arrival(1, h).wait_recv()
                mid_push(source, 3, h, 3, over)
            elif i > 1:
                pl.when(outer)(arrival(i, h).wait_recv)

        def to_x(h):
            part = halves[h]
            from_x[h, i] = push(source.at[:, part], block.at[:, part], gxy, (h, i), x_peer)

        def to_y(h):
            part = halves[h]
            from_y[h, i] = push(source.at[:, part], block.at[:, part], gxy, (2 + h, i), y_peer)

        ready(0)
        to_x(0)
        ready(1)
        to_y(1)
        to_x(1)
        to_y(0)
        if i == 0:
            for h in range(2):
                part = halves[h]
                sent.append(
                    sender(
                        source.at[:, part],
                        blocks.at[1, me_s, :, part],
                        gz[0].at[h, 1],
                        gz[1].at[h, 1],
                        near,
                    )
                )
                sent[-1].start()
                mid_push(source, 2, h, 2, over)

    def relay(i):
        from_x[0, i].wait_recv()
        part = blocks.at[i, s_x, :, lower]
        from_da[i] = push(part, part, gd, (0, i), y_peer)
        from_y[1, i].wait_recv()
        part = blocks.at[i, s_y, :, upper]
        from_db[i] = push(part, part, gd, (1, i), x_peer)

    def gathered(i):
        from_x[1, i].wait_recv()
        from_y[0, i].wait_recv()
        from_da[i].wait_recv()
        from_db[i].wait_recv()

    own_copy = pltpu.make_async_copy(normed_ref, blocks.at[0, me_s], own_sem)
    own_copy.start()
    spread(0)
    for copy in share:
        copy.wait()
    for place in range(n_sp):
        turned = jnp.transpose(share_in[place])
        lane = lax.broadcasted_iota(jnp.int32, turned.shape, 1)
        chosen = jnp.sum(jnp.where(lane == me_s, turned, 0.0), axis=1, keepdims=True)
        share_cols[place] = jnp.broadcast_to(chosen, (rows, LANES))

    ff = w_gate.shape[2]
    f_tile, d_tile = 256, min(512, width)
    count = n_sp * piece
    first_xs, first_ys, second_xs, second_ys = {}, {}, {}, {}
    slabs = ff // f_tile

    def swapped(k):
        w_swaps[k].wait_recv()

    def rise(i, step):
        tokens = blocks[i].reshape(count, width)
        for tile in (2 * step, 2 * step + 1):
            core, span = tile // slabs, pl.ds(tile % slabs * f_tile, f_tile)
            gate_part = jnp.dot(tokens, w_gate[core, :, span], preferred_element_type=jnp.float32)
            up_part = jnp.dot(tokens, w_up[core, :, span], preferred_element_type=jnp.float32)
            hidden_units[:, tile * f_tile : (tile + 1) * f_tile] = (
                gate_part * jax.nn.sigmoid(gate_part) * up_part
            ).astype(jnp.bfloat16)

    def fall(i, h):
        first = pl.multiple_of(across[i] * (2 * piece) + me_c * piece, piece)
        scale = share_cols[:, pl.ds(first, piece), :].reshape(count, LANES)[:, :1]
        units = hidden_units[...]
        for step in range(half // d_tile):
            begin = h * half + step * d_tile
            span = slice(begin, begin + d_tile)
            product = jnp.dot(
                units,
                w_down[:, :, span].reshape(2 * ff, d_tile),
                preferred_element_type=jnp.float32,
            )
            joined[i, :, :, span] = (
                (product * scale).astype(jnp.bfloat16).reshape(n_sp, piece, d_tile)
            )

    def depart(i, h):
        if h == 0:
            first_xs[1, i] = push(joined.at[i, s_d, :, lower], first_x.at[1, i], r1, (2, i), x_peer)
            first_xs[0, i] = push(joined.at[i, s_x, :, lower], first_x.at[0, i], r1, (0, i), x_peer)
        else:
            first_ys[1, i] = push(joined.at[i, s_d, :, upper], first_y.at[1, i], r1, (3, i), y_peer)
            first_ys[0, i] = push(joined.at[i, s_y, :, upper], first_y.at[0, i], r1, (1, i), y_peer)

    def turn(i):
        first_xs[1, i].wait_recv()
        relay_a[i] = (
            joined[i, s_y, :, :half].astype(jnp.float32) + first_x[1, i].astype(jnp.float32)
        ).astype(jnp.bfloat16)
        second_ys[i] = push(relay_a.at[i], second_y.at[i], r2, (0, i), y_peer)
        first_ys[1, i].wait_recv()
        relay_b[i] = (
            joined[i, s_x, :, half:].astype(jnp.float32) + first_y[1, i].astype(jnp.float32)
        ).astype(jnp.bfloat16)
        second_xs[i] = push(relay_b.at[i], second_x.at[i], r2, (1, i), x_peer)

    def finish(i):
        for copies in (first_xs, first_ys):
            copies[0, i].wait_recv()
        for copies in (second_xs, second_ys):
            copies[i].wait_recv()
        low = (
            joined[i, me_s, :, :half].astype(jnp.float32)
            + first_x[0, i].astype(jnp.float32)
            + second_y[i].astype(jnp.float32)
        )
        high = (
            joined[i, me_s, :, half:].astype(jnp.float32)
            + first_y[0, i].astype(jnp.float32)
            + second_x[i].astype(jnp.float32)
        )
        column[i] = jnp.concatenate([low, high], axis=1).astype(jnp.bfloat16)
        if i in (1, 3):
            copy = sender(
                column.at[i], last_in.at[me_z], rz[0].at[0, i], rz[1].at[0, me_z], z_peers[i - 1]
            )
            copy.start()
            sent.append(copy)
        elif i == 2:
            for h in range(2):
                pl.when(outer)(homeward[h].start)

    homeward, crossed = [], []
    for h in range(2):
        part = halves[h]
        homeward.append(
            sender(
                column.at[2, :, part],
                last_in.at[z_near, :, part],
                rz[0].at[h, 2],
                rz[1].at[h, z_near],
                near,
            )
        )
        crossed.append(
            sender(
                relay_c.at[:, part],
                last_in.at[me_z, :, part],
                rz[0].at[h, 2],
                rz[1].at[h, me_z],
                over,
            )
        )

    def cross(i):
        @pl.when(middle)
        def _():
            for h in range(2):
                span = slice(h * half, (h + 1) * half)
                part = last_in.at[me_z, :, halves[h]]
                sender(part, part, rz[0].at[h, 2], rz[1].at[h, me_z], near).wait_recv()
                relay_c[:, span] = (
                    column[i, :, span].astype(jnp.float32)
                    + last_in[me_z, :, span].astype(jnp.float32)
                ).astype(jnp.bfloat16)
                crossed[h].start()

    own_copy.wait()
    plan = (
        (relay, 0),
        (pass_on, 2, 0),
        (pass_on, 2, 1),
        (spread, 1),
        (gathered, 0),
        (swapped, 0),
        (swapped, 1),
        (rise, 0, 0),
        (relay, 1),
        (rise, 0, 1),
        (spread, 2),
        (pass_on, 3, 0),
        (pass_on, 3, 1),
        (rise, 0, 2),
        (swapped, 2),
        (fall, 0, 0),
        (fall, 0, 1),
        (gathered, 1),
        (rise, 1, 0),
        (relay, 2),
        (rise, 1, 1),
        (spread, 3),
        (rise, 1, 2),
        (fall, 1, 0),
        (fall, 1, 1),
        (gathered, 2),
        (rise, 2, 0),
        (rise, 2, 1),
        (relay, 3),
        (depart, 1, 0),
        (depart, 1, 1),
        (rise, 2, 2),
        (fall, 2, 0),
        (depart, 2, 0),
        (fall, 2, 1),
        (depart, 2, 1),
        (gathered, 3),
        (rise, 3, 0),
        (turn, 1),
        (rise, 3, 1),
        (rise, 3, 2),
        (fall, 3, 0),
        (depart, 3, 0),
        (fall, 3, 1),
        (depart, 3, 1),
        (turn, 2),
        (finish, 1),
        (turn, 3),
        (depart, 0, 0),
        (depart, 0, 1),
        (finish, 2),
        (finish, 3),
        (turn, 0),
        (cross, 2),
        (finish, 0),
    )
    for stage, *at in plan:
        stage(*at)
    total = own_ref[...].astype(jnp.float32) + column[0].astype(jnp.float32)
    def landed(h, z):
        if h is None:
            sender(column.at[0], last_in.at[z], rz[0].at[0, 0], rz[1].at[0, z], near).wait_recv()
        else:
            part = last_in.at[z, :, halves[h]]
            sender(part, part, rz[0].at[h, 0], rz[1].at[h, z], near).wait_recv()

    landed(None, z_near)
    total = total + last_in[z_near].astype(jnp.float32)

    @pl.when(outer)
    def _():
        landed(None, across[2])
        landed(None, z_far)

    @pl.when(middle)
    def _():
        landed(0, z_far)
        landed(1, z_far)
        last_in[me_z] = jnp.zeros(last_in.shape[1:], last_in.dtype)

    total = total + last_in[z_far].astype(jnp.float32)
    last = jnp.where(middle, me_z, across[2])
    total = total + last_in[pl.ds(last, 1)][0].astype(jnp.float32)
    out_ref[...] = total.astype(jnp.bfloat16)
    for copies in pair:
        for copy in copies:
            copy.wait_send()
    for copy in square_copies + w_swaps:
        copy.wait_send()

    @pl.when(outer)
    def _():
        for copy in list(inward.values()) + homeward:
            copy.wait_send()

    @pl.when(middle)
    def _():
        for copy in list(crossing.values()) + list(outward.values()) + mid_sent + crossed:
            copy.wait_send()

    for copy in sent:
        copy.wait_send()


def dense_local(
    lru_input,
    gate_input,
    documents,
    conv_taps,
    rate_weight,
    inlet_weight,
    decay_param,
    lru_gain,
    out_weight,
    residual,
    ffn_gain,
    routes,
    route_weights,
    w_gate,
    w_up,
    w_down,
):
    n_sp, n_tp = lax.axis_size("sp"), lax.axis_size("tp")
    n_z = n_tp // 2
    rows, channels = lru_input.shape
    width = residual.shape[1]
    ff = w_gate.shape[2]
    piece = rows // n_tp
    padded = -(-n_sp // 8) * 8
    vmem = pl.BlockSpec(memory_space=pltpu.VMEM)
    half = width // 2
    top = routes.shape[1]
    hbm = pl.BlockSpec(memory_space=pltpu.HBM)
    bf16, f32 = jnp.bfloat16, jnp.float32
    dma = pltpu.SemaphoreType.DMA
    rows_buffer = pltpu.VMEM((n_z, piece, width), bf16)
    half_buffer = pltpu.VMEM((n_z, piece, half), bf16)
    groups = pltpu.VMEM((n_z, n_sp, piece, width), bf16)
    square_buffer = pltpu.VMEM((n_z, 8, LANES), f32)
    shapes = (
        [(n_sp,)] * 8
        + [(2, n_z)] * 2
        + [(2, n_z + 2)] * 2
        + [(n_z,)] * 2
        + [(2, n_z + 2)] * 2
        + [(4, n_z)] * 2
        + [(2, n_z)] * 2
        + [(3,)] * 2
        + [(4, n_z)] * 2
        + [(2, n_z)] * 2
        + [(2, n_z)] * 2
    )
    return pl.pallas_call(
        functools.partial(layer_kernel, n_sp, n_tp),
        out_shape=pltpu.VMEM((piece, width), bf16),
        in_specs=[hbm] * 16,
        out_specs=vmem,
        scratch_shapes=[
            pltpu.VMEM((rows, channels), bf16),
            pltpu.VMEM((rows, channels), bf16),
            pltpu.VMEM((1, rows), jnp.int32),
            pltpu.VMEM(conv_taps.shape, bf16),
            pltpu.VMEM(rate_weight.shape, bf16),
            pltpu.VMEM(inlet_weight.shape, bf16),
            pltpu.VMEM((1, channels), f32),
            pltpu.VMEM((1, channels), f32),
            pltpu.VMEM((channels, width), bf16),
            pltpu.VMEM((1, width), f32),
            pltpu.VMEM((top, rows), jnp.int32),
            pltpu.VMEM((top, rows), f32),
            pltpu.VMEM((rows, LANES), jnp.int32),
            pltpu.VMEM((padded, rows), f32),
            pltpu.VMEM((16, channels), bf16),
            pltpu.VMEM((n_sp, 16, channels), bf16),
            pltpu.VMEM((8, LANES), jnp.int32),
            pltpu.VMEM((n_sp, 8, LANES), jnp.int32),
            pltpu.VMEM((8, channels), f32),
            pltpu.VMEM((n_sp, 8, channels), f32),
            pltpu.VMEM((n_sp, 8, channels), f32),
            pltpu.VMEM((n_sp, 8, channels), f32),
            pltpu.VMEM((n_sp, padded, rows), f32),
            pltpu.VMEM((rows, channels), f32),
            pltpu.VMEM((rows, channels), f32),
            pltpu.VMEM((n_tp, piece, width), bf16),
            rows_buffer,
            rows_buffer,
            rows_buffer,
            rows_buffer,
            rows_buffer,
            pltpu.VMEM((n_tp, 8, LANES), f32),
            square_buffer,
            square_buffer,
            square_buffer,
            pltpu.VMEM((piece, width), bf16),
            pltpu.VMEM((piece, width), bf16),
            pltpu.VMEM((piece, width), bf16),
            pltpu.VMEM((2, width, ff), bf16),
            pltpu.VMEM((2, width, ff), bf16),
            pltpu.VMEM((2, ff, width), bf16),
            pltpu.VMEM((n_sp, rows, LANES), f32),
            groups,
            pltpu.VMEM((n_sp * piece, 2 * ff), bf16),
            groups,
            pltpu.VMEM((2, n_z, piece, half), bf16),
            pltpu.VMEM((2, n_z, piece, half), bf16),
            half_buffer,
            half_buffer,
            half_buffer,
            half_buffer,
            pltpu.VMEM((piece, width), bf16),
            rows_buffer,
            rows_buffer,
            dma((12,)),
            dma,
            dma((3,)),
            dma,
        ]
        + [dma(shape) for shape in shapes],
        compiler_params=pltpu.CompilerParams(
            collective_id=0, has_side_effects=True, vmem_limit_bytes=48 * 2**20
        ),
    )(
        *(pltpu.with_memory_space_constraint(operand, pltpu.HBM) for operand in (
        lru_input,
        gate_input,
        documents[None, :],
        conv_taps,
        rate_weight,
        inlet_weight,
        decay_param[None, :],
        lru_gain[None, :],
        out_weight,
        residual,
        ffn_gain[None, :],
        routes.T,
        route_weights.T,
        w_gate[0],
        w_up[0],
        w_down[0],
        ))
    )


def solution(mesh):
    n_sp, n_tp = mesh.shape["sp"], mesh.shape["tp"]
    body = dense_local if n_sp == 4 and n_tp == 8 else local
    return jax.shard_map(
        body,
        mesh=mesh,
        in_specs=(
            P("sp", "tp"),
            P("sp", "tp"),
            P("sp"),
            P(None, "tp"),
            P("tp", None, None),
            P("tp", None, None),
            P("tp"),
            P("tp"),
            P("tp", None),
            P("sp", None),
            P(),
            P("sp", None),
            P("sp", None),
            P("sp", None, "tp"),
            P("sp", None, "tp"),
            P("sp", "tp", None),
        ),
        out_specs=P(("sp", "tp"), None),
        check_vma=False,
    )
```

```python
import functools

import jax
import jax.numpy as jnp
from jax import lax
from jax.experimental import pallas as pl
from jax.experimental.pallas import tpu as pltpu
from jax.sharding import PartitionSpec as P

D_RNN = 2048


EPSILON = 1e-06
RATE_SCALE = 8.0


def shifted(block, axis, distance):
    devices = range(lax.axis_size(axis))
    route = [(i - distance, i) for i in devices if i - distance in devices]
    return lax.ppermute(block, axis, route)


def carried_in(value, axis, join, neutral):
    count, mine = (lax.axis_size(axis), lax.axis_index(axis))
    pieces = jax.tree.map(lambda part: lax.all_gather(part, axis), value)
    so_far = jax.tree.map(
        lambda part, zero: jnp.full_like(part, 0) + jnp.asarray(zero, part.dtype), value, neutral
    )

    def hop(position, so_far):
        longer = join(so_far, jax.tree.map(lambda part: part[position], pieces))
        return jax.tree.map(lambda new, old: jnp.where(position < mine, new, old), longer, so_far)

    return lax.fori_loop(0, count - 1, hop, so_far)


def join_runs(earlier_run, later_run):
    return (earlier_run[0] * later_run[0], later_run[0] * earlier_run[1] + later_run[1])


def slot_targets(route_block, expert_count, capacity):
    flat_routes = route_block.reshape(-1)
    onehot = (flat_routes[:, None] == jnp.arange(expert_count, dtype=jnp.int32)[None, :]).astype(
        jnp.int32
    )
    earlier_hits = jnp.cumsum(onehot, axis=0) - onehot
    slot_index = jnp.sum(earlier_hits * onehot, axis=1)
    return (flat_routes * capacity + slot_index).reshape(route_block.shape)


def pick_matrix(targets, slot_total):
    slot_hits = targets[None, :, :] == jnp.arange(slot_total, dtype=jnp.int32)[:, None, None]
    return jnp.sum(slot_hits.astype(jnp.int32), axis=2).astype(jnp.bfloat16)


def rms_rows(row_block, gain_vector):
    floated = row_block.astype(jnp.float32)
    inverse_rms = lax.rsqrt(jnp.mean(floated * floated, axis=1, keepdims=True) + EPSILON)
    return (floated * inverse_rms * gain_vector[None, :]).astype(jnp.bfloat16)


def expert_apply(row_piece, gate_weight, up_weight, down_weight):
    gate_part = jnp.dot(row_piece, gate_weight, preferred_element_type=jnp.float32)
    up_part = jnp.dot(row_piece, up_weight, preferred_element_type=jnp.float32)
    hidden_units = (jax.nn.silu(gate_part) * up_part).astype(jnp.bfloat16)
    return jnp.dot(hidden_units, down_weight, preferred_element_type=jnp.float32)


def local(
    lru_input,
    gate_input,
    documents,
    conv_taps,
    rate_weight,
    inlet_weight,
    decay_param,
    lru_gain,
    out_weight,
    residual,
    ffn_gain,
    routes,
    route_weights,
    w_gate,
    w_up,
    w_down,
):
    positions = lru_input.shape[0]
    channels = lru_input.shape[1]
    model_width = residual.shape[1]
    reach_back = conv_taps.shape[0] - 1
    tail_rows, tail_docs = shifted(
        (lru_input[positions - reach_back :], documents[positions - reach_back :] + 1), "sp", 1
    )
    prior_docs = jnp.concatenate([tail_docs - 1, documents])
    padded_input = jnp.concatenate([tail_rows, lru_input], axis=0)
    conv_sum = jnp.zeros((positions, channels), jnp.float32)
    for tap_index in range(reach_back + 1):
        same_doc = (prior_docs[tap_index : tap_index + positions] == documents).astype(jnp.float32)[
            :, None
        ]
        conv_sum = (
            conv_sum
            + padded_input[tap_index : tap_index + positions].astype(jnp.float32)
            * conv_taps[tap_index].astype(jnp.float32)[None, :]
            * same_doc
        )
    convolved = conv_sum.astype(jnp.bfloat16)
    grouped = convolved.reshape(positions, rate_weight.shape[0], rate_weight.shape[1])
    rate_gate = jax.nn.sigmoid(
        jnp.einsum(
            "tnc,ncd->tnd", grouped, rate_weight, preferred_element_type=jnp.float32
        ).reshape(positions, channels)
    )
    inlet_gate = jax.nn.sigmoid(
        jnp.einsum(
            "tnc,ncd->tnd", grouped, inlet_weight, preferred_element_type=jnp.float32
        ).reshape(positions, channels)
    )
    log_decay = -RATE_SCALE * rate_gate * jax.nn.softplus(-decay_param)[None, :]
    starts = (prior_docs[reach_back - 1 : reach_back - 1 + positions] != documents)[:, None]
    decay_step = jnp.where(starts, 0.0, jnp.exp(log_decay))
    norm_factor = jnp.where(starts, 1.0, jnp.sqrt(-jnp.expm1(2.0 * log_decay)))
    drive_term = norm_factor * inlet_gate * convolved.astype(jnp.float32)
    decay_run, local_state = lax.associative_scan(join_runs, (decay_step, drive_term), axis=0)
    carried = carried_in(
        (decay_run[positions - 1], local_state[positions - 1]),
        "sp",
        join_runs,
        (jnp.ones((channels,), jnp.float32), jnp.zeros((channels,), jnp.float32)),
    )
    hidden_state = local_state + decay_run * carried[1][None, :]
    square_sums = lax.psum(jnp.sum(hidden_state * hidden_state, axis=1), "tp")
    inverse_rms = lax.rsqrt(square_sums[:, None] / D_RNN + EPSILON)
    mixer_rows = (
        hidden_state * inverse_rms * lru_gain[None, :] * jax.nn.gelu(gate_input.astype(jnp.float32))
    ).astype(jnp.bfloat16)
    tp_count = lax.axis_size("tp")
    tp_here = lax.axis_index("tp")
    expert_count = lax.axis_size("sp")
    route_rows = positions // tp_count
    top_count = routes.shape[1]
    capacity = 2 * top_count * route_rows // expert_count
    slot_total = expert_count * capacity
    projected = lax.psum_scatter(
        jnp.dot(mixer_rows, out_weight, preferred_element_type=jnp.float32).astype(jnp.bfloat16),
        "tp",
        scatter_dimension=0,
        tiled=True,
    ).astype(jnp.float32)
    own_rows = (
        lax.dynamic_slice_in_dim(residual, tp_here * route_rows, route_rows, 0).astype(jnp.float32)
        + projected
    ).astype(jnp.bfloat16)
    own_routes = lax.dynamic_slice_in_dim(routes, tp_here * route_rows, route_rows, 0)
    targets = slot_targets(own_routes, expert_count, capacity)
    outgoing = jnp.dot(
        pick_matrix(targets, slot_total),
        rms_rows(own_rows, ffn_gain),
        preferred_element_type=jnp.float32,
    ).astype(jnp.bfloat16)
    arrived = lax.all_to_all(
        outgoing.reshape(expert_count, capacity, model_width),
        "sp",
        split_axis=0,
        concat_axis=0,
        tiled=True,
    )
    partial_out = expert_apply(
        lax.all_gather(arrived.reshape(slot_total, model_width), "tp", axis=0, tiled=True),
        w_gate[0],
        w_up[0],
        w_down[0],
    )
    expert_out = lax.psum_scatter(
        partial_out.astype(jnp.bfloat16), "tp", scatter_dimension=0, tiled=True
    )
    returned = lax.all_to_all(
        expert_out.reshape(expert_count, capacity, model_width),
        "sp",
        split_axis=0,
        concat_axis=0,
        tiled=True,
    )
    picked = returned.reshape(slot_total, model_width)[targets.reshape(-1)].astype(jnp.float32)
    picked = picked.reshape(route_rows, top_count, model_width)
    own_weights = lax.dynamic_slice_in_dim(route_weights, tp_here * route_rows, route_rows, 0)
    routed = jnp.sum(picked * own_weights[:, :, None], axis=1)
    return (own_rows.astype(jnp.float32) + routed).astype(jnp.bfloat16)


MESH = pl.DeviceIdType.MESH
LANES = 128
GELU_SCALE = 0.7978845608028654


def sender(source, target, send_sem, recv_sem, peer):
    return pltpu.make_async_remote_copy(
        src_ref=source,
        dst_ref=target,
        send_sem=send_sem,
        recv_sem=recv_sem,
        device_id=peer,
        device_id_type=MESH,
    )


def greet(peers):
    barrier = pltpu.get_barrier_semaphore()
    for peer in peers:
        pl.semaphore_signal(barrier, inc=1, device_id=peer, device_id_type=MESH)
    pl.semaphore_wait(barrier, len(peers))


def one_minus_exp(value):
    series = 1.0 + value * (1.0 / 6.0)
    for order in (5.0, 4.0, 3.0, 2.0):
        series = 1.0 + value * (1.0 / order) * series
    return jnp.where(value > -0.25, -value * series, 1.0 - jnp.exp(value))


def down_by(block, distance, filler):
    count = block.shape[0]
    if distance % 8 == 0:
        top = jnp.full((distance, block.shape[1]), filler, block.dtype)
        return jnp.concatenate([top, block[: count - distance]], axis=0)
    row = lax.broadcasted_iota(jnp.int32, block.shape, 0)
    return jnp.where(row >= distance, pltpu.roll(block, distance, 0), filler)


LATE = 8


def layer_kernel(
    n_sp,
    n_tp,
    lru_hbm,
    gate_hbm,
    docs_hbm,
    taps_hbm,
    rate_hbm,
    inlet_hbm,
    decay_hbm,
    gain_hbm,
    out_w_hbm,
    residual_hbm,
    ffn_hbm,
    routes_hbm,
    shares_hbm,
    w_gate_hbm,
    w_up_hbm,
    w_down_hbm,
    out_ref,
    lru_ref,
    gate_ref,
    docs_row,
    taps_ref,
    rate_ref,
    inlet_ref,
    decay_ref,
    gain_ref,
    out_w_ref,
    ffn_ref,
    routes_ref,
    route_w_ref,
    docs_ref,
    weights_ref,
    edge_out,
    edge_in,
    mark_out,
    mark_in,
    carry_out,
    carry_in,
    head_a,
    head_b,
    share_in,
    run_a,
    run_b,
    parts,
    pair_in,
    z_out,
    z_in,
    z_sum,
    z_across,
    squares,
    square_pair,
    square_out,
    square_in,
    res_rows,
    own_ref,
    normed_ref,
    w_gate,
    w_up,
    w_down,
    share_cols,
    blocks,
    hidden_units,
    joined,
    first_x,
    first_y,
    second_x,
    second_y,
    relay_a,
    relay_b,
    relay_c,
    column,
    last_in,
    load_sem,
    res_sem,
    w_sem,
    own_sem,
    edge_s,
    edge_r,
    mark_s,
    mark_r,
    carry_s,
    carry_r,
    share_s,
    share_r,
    pair_s,
    pair_r,
    z_s,
    z_r,
    sq_s,
    sq_r,
    gz_s,
    gz_r,
    gxy_s,
    gxy_r,
    gd_s,
    gd_r,
    wp_s,
    wp_r,
    r1_s,
    r1_r,
    r2_s,
    r2_r,
    rz_s,
    rz_r,
):
    me_s, me_t = lax.axis_index("sp"), lax.axis_index("tp")
    n_z = n_tp // 2
    me_z, me_c = me_t // 2, me_t % 2
    rows, channels = lru_ref.shape
    width = out_w_ref.shape[1]
    piece = rows // n_tp
    pairs = (
        (lru_hbm, lru_ref),
        (docs_hbm, docs_row),
        (taps_hbm, taps_ref),
        (rate_hbm, rate_ref),
        (inlet_hbm, inlet_ref),
        (decay_hbm, decay_ref),
        (routes_hbm, routes_ref),
        (shares_hbm, route_w_ref),
        (out_w_hbm, out_w_ref),
        (gate_hbm, gate_ref),
        (gain_hbm, gain_ref),
        (ffn_hbm, ffn_ref),
    )
    loads = [
        pltpu.make_async_copy(source, target, load_sem.at[k])
        for k, (source, target) in enumerate(pairs)
    ]
    for copy in loads:
        copy.start()
    residual_copy = pltpu.make_async_copy(
        residual_hbm.at[pl.ds(pl.multiple_of(me_t * piece, piece), piece)], res_rows, res_sem
    )
    residual_copy.start()
    w_loads = [
        pltpu.make_async_copy(source, target, w_sem.at[k])
        for k, (source, target) in enumerate(
            (
                (w_gate_hbm, w_gate.at[me_c]),
                (w_up_hbm, w_up.at[me_c]),
                (w_down_hbm, w_down.at[me_c]),
            )
        )
    ]
    s_x = me_s + 1 - 2 * (me_s % 2)
    s_y = (me_s + 2) % n_sp
    s_d = n_sp - 1 - me_s
    x_peer, y_peer = (s_x, me_t), (s_y, me_t)
    partner = (me_s, me_z * 2 + 1 - me_c)
    sp_peers = [((me_s + k) % n_sp, me_t) for k in range(1, n_sp)]
    z_near, z_far = me_z + 1 - 2 * (me_z % 2), n_z - 1 - me_z
    upper_side = me_z // 2
    across = (me_z, z_near, 2 - upper_side, 3 - 3 * upper_side)
    middle = (me_z + 1) // 2 % 2 == 1
    outer = (me_z + 1) // 2 % 2 == 0
    near, over = (me_s, z_near * 2 + me_c), (me_s, z_far * 2 + me_c)
    z_peers = [(me_s, across[k] * 2 + me_c) for k in range(1, n_z)]
    greeted = sp_peers + z_peers + [partner]
    barrier = pltpu.get_barrier_semaphore()
    for peer in greeted:
        pl.semaphore_signal(barrier, inc=1, device_id=peer, device_id_type=MESH)
    for k in range(6):
        loads[k].wait()
    for copy in w_loads:
        copy.start()
    docs = jnp.transpose(jnp.broadcast_to(docs_row[...], (8, rows)))
    docs = jnp.broadcast_to(docs[:, :1], (rows, LANES))
    docs_ref[...] = docs
    lane8 = lax.broadcasted_iota(jnp.int32, (8, LANES), 1)
    mark_out[...] = jnp.where(lane8 == 0, docs[:8], docs[rows - 8 :])
    edge_out[0:16] = lru_ref[0:16]
    edge_out[16:32] = lru_ref[rows - 16 :]
    taps = taps_ref[...].astype(jnp.float32)
    reach = taps.shape[0] - 1

    def gates(convolved, starts, group):
        span = slice(group * LANES, (group + 1) * LANES)
        rate = jax.nn.sigmoid(
            jnp.dot(convolved, rate_ref[group], preferred_element_type=jnp.float32)
        )
        inlet = jax.nn.sigmoid(
            jnp.dot(convolved, inlet_ref[group], preferred_element_type=jnp.float32)
        )
        minus = -decay_ref[:, span]
        soft = jnp.maximum(minus, 0.0) + jnp.log1p(jnp.exp(-jnp.abs(minus)))
        log_decay = -RATE_SCALE * rate * soft
        step = jnp.where(starts, 0.0, jnp.exp(log_decay))
        factor = jnp.where(starts, 1.0, jnp.sqrt(one_minus_exp(2.0 * log_decay)))
        return step, factor * inlet * convolved.astype(jnp.float32)

    body = rows - 8
    starts = docs[7 : 7 + body] != docs[8:]
    for group in range(channels // LANES):
        span = slice(group * LANES, (group + 1) * LANES)
        long = lru_ref[:, span].astype(jnp.float32)
        total = jnp.zeros((body, LANES), jnp.float32)
        for tap in range(reach + 1):
            first = 8 - reach + tap
            same = docs[first : first + body] == docs[8:]
            total = total + jnp.where(same, long[first : first + body], 0.0) * taps[tap : tap + 1, span]
        step, state = gates(total.astype(jnp.bfloat16), starts, group)
        distance = 1
        while distance < body:
            state = state + step * down_by(state, distance, 0.0)
            step = step * down_by(step, distance, 1.0)
            distance *= 2
        run_a[8:, span] = step
        run_b[8:, span] = state
        carry_out[:, span] = jnp.concatenate(
            [step[body - 1 :], state[body - 1 :], jnp.zeros((6, LANES), jnp.float32)], axis=0
        )
    pl.semaphore_wait(barrier, len(greeted))
    carry = []
    for k, peer in enumerate(sp_peers):
        carry += [
            sender(carry_out, carry_in.at[me_s], carry_s.at[k], carry_r.at[k], peer),
            sender(mark_out, mark_in.at[me_s], mark_s.at[k], mark_r.at[k], peer),
            sender(edge_out, edge_in.at[me_s], edge_s.at[k], edge_r.at[k], peer),
        ]
    for copy in carry:
        copy.start()
    w_swaps = [
        sender(part.at[me_c], part.at[me_c], wp_s.at[k], wp_r.at[k], partner)
        for k, part in enumerate((w_gate, w_up, w_down))
    ]
    carry_in[pl.ds(me_s, 1)] = carry_out[...][None]
    mark_in[pl.ds(me_s, 1)] = mark_out[...][None]
    edge_in[pl.ds(me_s, 1)] = edge_out[...][None]
    loads[6].wait()
    loads[7].wait()
    expert = lax.broadcasted_iota(jnp.int32, weights_ref.shape, 0)
    shares = jnp.zeros(weights_ref.shape, jnp.float32)
    for k in range(routes_ref.shape[0]):
        shares = shares + jnp.where(
            routes_ref[k : k + 1] == expert, route_w_ref[k : k + 1], 0.0
        )
    weights_ref[...] = shares
    share = [
        sender(weights_ref, share_in.at[me_s], share_s.at[k], share_r.at[k], peer)
        for k, peer in enumerate(sp_peers)
    ]
    for copy in share:
        copy.start()
    share_in[pl.ds(me_s, 1)] = shares[None]
    for k in (9, 10, 11):
        loads[k].wait()
    raw = gate_ref[...].astype(jnp.float32)
    gelu = 0.5 * raw * (1.0 + jnp.tanh(GELU_SCALE * (raw + 0.044715 * raw * raw * raw)))
    gelu = gelu * gain_ref[...]
    for copy in carry:
        copy.wait()
    xs, now, prior = [], [], []
    for place in range(n_sp):
        marks = mark_in[place]
        now.append(jnp.broadcast_to(marks[:, 0:1], (8, LANES)))
        if place == 0:
            prior.append(jnp.full((8, LANES), -1, jnp.int32))
        else:
            prior.append(jnp.broadcast_to(mark_in[place - 1][:, 1:2], (8, LANES)))
        xs.append(
            jnp.concatenate(
                [
                    edge_in[max(place - 1, 0)].astype(jnp.float32)[24:],
                    edge_in[place].astype(jnp.float32)[:8],
                ],
                axis=0,
            )
        )
    both = [jnp.concatenate([prior[p], now[p]], axis=0) for p in range(n_sp)]
    head_starts = jnp.concatenate([both[p][7:15] != now[p] for p in range(n_sp)], axis=0)
    in_tile = lax.broadcasted_iota(jnp.int32, (8 * n_sp, LANES), 0) % 8
    for group in range(channels // LANES):
        span = slice(group * LANES, (group + 1) * LANES)
        sums = []
        for place in range(n_sp):
            total = jnp.zeros((8, LANES), jnp.float32)
            for tap in range(reach + 1):
                first = 8 - reach + tap
                same = both[place][first : first + 8] == now[place]
                total = total + (
                    jnp.where(same, xs[place][first : first + 8, span], 0.0)
                    * taps[tap : tap + 1, span]
                )
            sums.append(total)
        step, state = gates(jnp.concatenate(sums, axis=0).astype(jnp.bfloat16), head_starts, group)
        for distance in (1, 2, 4):
            inside = in_tile >= distance
            state = state + step * jnp.where(inside, pltpu.roll(state, distance, 0), 0.0)
            step = step * jnp.where(inside, pltpu.roll(step, distance, 0), 1.0)
        head_a[:, :, span] = step.reshape(n_sp, 8, LANES)
        head_b[:, :, span] = state.reshape(n_sp, 8, LANES)
    carried = jnp.zeros((1, channels), jnp.float32)
    for place in range(n_sp - 1):
        entered = head_b[place][7:] + head_a[place][7:] * carried
        tile = carry_in[place]
        carried = jnp.where(place < me_s, tile[1:2] + tile[0:1] * entered, carried)
    top = head_b[pl.ds(me_s, 1)][0] + head_a[pl.ds(me_s, 1)][0] * carried
    hidden = jnp.concatenate([top, run_b[8:] + run_a[8:] * top[7:]], axis=0)
    row_squares = jnp.sum(hidden * hidden, axis=1, keepdims=True)
    for place in range(n_tp):
        packed = jnp.zeros((8, LANES), jnp.float32)
        for j in range(piece // 8):
            first = place * piece + j * 8
            packed = jnp.where(lane8 == j, row_squares[first : first + 8], packed)
        squares[place] = packed
    loads[LATE].wait()
    mixer = (hidden * gelu).astype(jnp.bfloat16)
    tile_width = min(512, width)
    for first in range(0, width, tile_width):
        span = slice(first, first + tile_width)
        product = jnp.dot(mixer, out_w_ref[:, span], preferred_element_type=jnp.float32)
        parts[:, :, span] = product.astype(jnp.bfloat16).reshape(n_tp, piece, tile_width)

    half = width // 2
    halves = (pl.ds(0, half), pl.ds(half, half))
    pair = []
    for i in (3, 2, 1, 0):
        theirs = across[i] * 2 + 1 - me_c
        pair.append(
            (
                sender(squares.at[theirs], square_pair.at[i], pair_s.at[1, i], pair_r.at[1, i], partner),
                sender(parts.at[theirs], pair_in.at[i], pair_s.at[0, i], pair_r.at[0, i], partner),
            )
        )
        for copy in pair[-1]:
            copy.start()
    square_copies = []
    inward = {}
    for i in (3, 2, 1):
        for h in range(2):
            inward[i, h] = sender(
                z_out.at[i, :, halves[h]], z_in.at[i, :, halves[h]], z_s.at[h, i], z_r.at[h, i], near
            )
    for n, i in enumerate((3, 2, 1, 0)):
        mine = across[i] * 2 + me_c
        for copy in pair[n]:
            copy.wait_recv()
        square_out[i] = squares[mine] + square_pair[i]
        if i > 0:
            copy = sender(
                square_out.at[i], square_in.at[me_z], sq_s.at[i], sq_r.at[me_z], z_peers[i - 1]
            )
            copy.start()
            square_copies.append(copy)
        z_out[i] = (
            parts[mine].astype(jnp.float32) + pair_in[i].astype(jnp.float32)
        ).astype(jnp.bfloat16)

        if i > 0:

            @pl.when(outer)
            def _():
                for h in range(2):
                    inward[i, h].start()

    for k in range(3):
        w_loads[k].wait()
        w_swaps[k].start()
    crossing, outward = {}, {}
    for i in (3, 2):
        for h in range(2):
            crossing[i, h] = sender(
                z_sum.at[i, :, halves[h]], z_across.at[i, :, halves[h]], z_s.at[h, i + 2], z_r.at[h, i + 2], over
            )
    for h in range(2):
        outward[h] = sender(
            z_sum.at[1, :, halves[h]], z_in.at[0, :, halves[h]], z_s.at[h, 0], z_r.at[h, 0], near
        )

    @pl.when(middle)
    def _():
        def add_up(target, i, h, received):
            span = slice(h * half, (h + 1) * half)
            target[i, :, span] = (
                z_out[i, :, span].astype(jnp.float32) + received[:, span].astype(jnp.float32)
            ).astype(jnp.bfloat16)

        for i, h in ((3, 0), (3, 1), (2, 0)):
            inward[i, h].wait_recv()
            add_up(z_sum, i, h, z_in.at[i])
            crossing[i, h].start()
        for h in range(2):
            if h == 1:
                inward[2, 1].wait_recv()
                add_up(z_sum, 2, 1, z_in.at[2])
                crossing[2, 1].start()
            crossing[3, h].wait_recv()
            add_up(z_sum, 1, h, z_across.at[3])
            outward[h].start()
        for h in range(2):
            inward[1, h].wait_recv()
            add_up(z_sum, 0, h, z_in.at[1])
        for h in range(2):
            crossing[2, h].wait_recv()
        z_in[0] = (z_sum[0].astype(jnp.float32) + z_across[2].astype(jnp.float32)).astype(jnp.bfloat16)
        z_sum[0] = z_in[0]

    @pl.when(outer)
    def _():
        for h in range(2):
            outward[h].wait_recv()
        z_sum[0] = (z_out[0].astype(jnp.float32) + z_in[0].astype(jnp.float32)).astype(jnp.bfloat16)

    summed = z_sum[0].astype(jnp.float32)
    square_sum = square_out[0]
    for k in range(1, n_z):
        from_z = (me_z + k) % n_z
        sender(
            square_out.at[0], square_in.at[from_z], sq_s.at[0], sq_r.at[from_z], near
        ).wait_recv()
        square_sum = square_sum + square_in[pl.ds(from_z, 1)][0]
    square_sum = jnp.concatenate(
        [square_sum[:, j : j + 1] for j in range(piece // 8)], axis=0
    )
    inverse = lax.rsqrt(square_sum / (channels * n_tp) + EPSILON)
    residual_copy.wait()
    own = (res_rows[...].astype(jnp.float32) + summed * inverse).astype(jnp.bfloat16)
    own_ref[...] = own
    floated = own.astype(jnp.float32)
    inverse = lax.rsqrt(jnp.mean(floated * floated, axis=1, keepdims=True) + EPSILON)
    normed_ref[...] = (floated * inverse * ffn_ref[...]).astype(jnp.bfloat16)

    lower, upper = halves
    sent = []

    def push(source, target, sems, slot, peer):
        copy = sender(source, target, sems[0].at[slot], sems[1].at[slot], peer)
        copy.start()
        sent.append(copy)
        return copy

    gz, gxy, gd = (gz_s, gz_r), (gxy_s, gxy_r), (gd_s, gd_r)
    r1, r2, rz = (r1_s, r1_r), (r2_s, r2_r), (rz_s, rz_r)
    from_x, from_y, from_da, from_db = {}, {}, {}, {}
    mid_sent = []

    def arrival(i, h):
        part = blocks.at[i, me_s, :, halves[h]]
        return sender(part, part, gz[0].at[h, i], gz[1].at[h, i], near)

    def mid_push(source, i, h, slot, peer):
        part = blocks.at[i, me_s, :, halves[h]]
        copy = sender(source.at[:, halves[h]], part, gz[0].at[h, slot], gz[1].at[h, i], peer)
        pl.when(middle)(copy.start)
        mid_sent.append(copy)

    def pass_on(i, h):
        pl.when(middle)(arrival(i, h).wait_recv)
        mid_push(blocks.at[i, me_s], i, h, i + 2, near)

    def spread(i):
        block = blocks.at[i, me_s]
        source = normed_ref if i == 0 else block

        def ready(h):
            if i == 1:
                arrival(1, h).wait_recv()
                mid_push(source, 3, h, 3, over)
            elif i > 1:
                pl.when(outer)(arrival(i, h).wait_recv)

        def to_x(h):
            part = halves[h]
            from_x[h, i] = push(source.at[:, part], block.at[:, part], gxy, (h, i), x_peer)

        def to_y(h):
            part = halves[h]
            from_y[h, i] = push(source.at[:, part], block.at[:, part], gxy, (2 + h, i), y_peer)

        ready(0)
        to_x(0)
        ready(1)
        to_y(1)
        to_x(1)
        to_y(0)
        if i == 0:
            for h in range(2):
                part = halves[h]
                sent.append(
                    sender(
                        source.at[:, part],
                        blocks.at[1, me_s, :, part],
                        gz[0].at[h, 1],
                        gz[1].at[h, 1],
                        near,
                    )
                )
                sent[-1].start()
                mid_push(source, 2, h, 2, over)

    def relay(i):
        from_x[0, i].wait_recv()
        part = blocks.at[i, s_x, :, lower]
        from_da[i] = push(part, part, gd, (0, i), y_peer)
        from_y[1, i].wait_recv()
        part = blocks.at[i, s_y, :, upper]
        from_db[i] = push(part, part, gd, (1, i), x_peer)

    def gathered(i):
        from_x[1, i].wait_recv()
        from_y[0, i].wait_recv()
        from_da[i].wait_recv()
        from_db[i].wait_recv()

    own_copy = pltpu.make_async_copy(normed_ref, blocks.at[0, me_s], own_sem)
    own_copy.start()
    spread(0)
    for copy in share:
        copy.wait()
    for place in range(n_sp):
        turned = jnp.transpose(share_in[place])
        lane = lax.broadcasted_iota(jnp.int32, turned.shape, 1)
        chosen = jnp.sum(jnp.where(lane == me_s, turned, 0.0), axis=1, keepdims=True)
        share_cols[place] = jnp.broadcast_to(chosen, (rows, LANES))

    ff = w_gate.shape[2]
    f_tile, d_tile = 256, min(512, width)
    count = n_sp * piece
    first_xs, first_ys, second_xs, second_ys = {}, {}, {}, {}
    slabs = ff // f_tile

    def swapped(k):
        w_swaps[k].wait_recv()

    def rise(i, step):
        tokens = blocks[i].reshape(count, width)
        for tile in (2 * step, 2 * step + 1):
            core, span = tile // slabs, pl.ds(tile % slabs * f_tile, f_tile)
            gate_part = jnp.dot(tokens, w_gate[core, :, span], preferred_element_type=jnp.float32)
            up_part = jnp.dot(tokens, w_up[core, :, span], preferred_element_type=jnp.float32)
            hidden_units[:, tile * f_tile : (tile + 1) * f_tile] = (
                gate_part * jax.nn.sigmoid(gate_part) * up_part
            ).astype(jnp.bfloat16)

    def fall(i, h):
        first = pl.multiple_of(across[i] * (2 * piece) + me_c * piece, piece)
        scale = share_cols[:, pl.ds(first, piece), :].reshape(count, LANES)[:, :1]
        units = hidden_units[...]
        for step in range(half // d_tile):
            begin = h * half + step * d_tile
            span = slice(begin, begin + d_tile)
            product = jnp.dot(
                units,
                w_down[:, :, span].reshape(2 * ff, d_tile),
                preferred_element_type=jnp.float32,
            )
            joined[i, :, :, span] = (
                (product * scale).astype(jnp.bfloat16).reshape(n_sp, piece, d_tile)
            )

    def depart(i, h):
        if h == 0:
            first_xs[1, i] = push(joined.at[i, s_d, :, lower], first_x.at[1, i], r1, (2, i), x_peer)
            first_xs[0, i] = push(joined.at[i, s_x, :, lower], first_x.at[0, i], r1, (0, i), x_peer)
        else:
            first_ys[1, i] = push(joined.at[i, s_d, :, upper], first_y.at[1, i], r1, (3, i), y_peer)
            first_ys[0, i] = push(joined.at[i, s_y, :, upper], first_y.at[0, i], r1, (1, i), y_peer)

    def turn(i):
        first_xs[1, i].wait_recv()
        relay_a[i] = (
            joined[i, s_y, :, :half].astype(jnp.float32) + first_x[1, i].astype(jnp.float32)
        ).astype(jnp.bfloat16)
        second_ys[i] = push(relay_a.at[i], second_y.at[i], r2, (0, i), y_peer)
        first_ys[1, i].wait_recv()
        relay_b[i] = (
            joined[i, s_x, :, half:].astype(jnp.float32) + first_y[1, i].astype(jnp.float32)
        ).astype(jnp.bfloat16)
        second_xs[i] = push(relay_b.at[i], second_x.at[i], r2, (1, i), x_peer)

    def finish(i):
        for copies in (first_xs, first_ys):
            copies[0, i].wait_recv()
        for copies in (second_xs, second_ys):
            copies[i].wait_recv()
        low = (
            joined[i, me_s, :, :half].astype(jnp.float32)
            + first_x[0, i].astype(jnp.float32)
            + second_y[i].astype(jnp.float32)
        )
        high = (
            joined[i, me_s, :, half:].astype(jnp.float32)
            + first_y[0, i].astype(jnp.float32)
            + second_x[i].astype(jnp.float32)
        )
        column[i] = jnp.concatenate([low, high], axis=1).astype(jnp.bfloat16)
        if i in (1, 3):
            copy = sender(
                column.at[i], last_in.at[me_z], rz[0].at[0, i], rz[1].at[0, me_z], z_peers[i - 1]
            )
            copy.start()
            sent.append(copy)
        elif i == 2:
            for h in range(2):
                pl.when(outer)(homeward[h].start)

    homeward, crossed = [], []
    for h in range(2):
        part = halves[h]
        homeward.append(
            sender(
                column.at[2, :, part],
                last_in.at[z_near, :, part],
                rz[0].at[h, 2],
                rz[1].at[h, z_near],
                near,
            )
        )
        crossed.append(
            sender(
                relay_c.at[:, part],
                last_in.at[me_z, :, part],
                rz[0].at[h, 2],
                rz[1].at[h, me_z],
                over,
            )
        )

    def cross(i):
        @pl.when(middle)
        def _():
            for h in range(2):
                span = slice(h * half, (h + 1) * half)
                part = last_in.at[me_z, :, halves[h]]
                sender(part, part, rz[0].at[h, 2], rz[1].at[h, me_z], near).wait_recv()
                relay_c[:, span] = (
                    column[i, :, span].astype(jnp.float32)
                    + last_in[me_z, :, span].astype(jnp.float32)
                ).astype(jnp.bfloat16)
                crossed[h].start()

    own_copy.wait()
    plan = (
        (relay, 0),
        (pass_on, 2, 0),
        (pass_on, 2, 1),
        (spread, 1),
        (gathered, 0),
        (swapped, 0),
        (swapped, 1),
        (rise, 0, 0),
        (relay, 1),
        (rise, 0, 1),
        (spread, 2),
        (pass_on, 3, 0),
        (pass_on, 3, 1),
        (rise, 0, 2),
        (swapped, 2),
        (fall, 0, 0),
        (fall, 0, 1),
        (gathered, 1),
        (rise, 1, 0),
        (relay, 2),
        (rise, 1, 1),
        (spread, 3),
        (rise, 1, 2),
        (fall, 1, 0),
        (fall, 1, 1),
        (gathered, 2),
        (rise, 2, 0),
        (rise, 2, 1),
        (relay, 3),
        (depart, 1, 0),
        (depart, 1, 1),
        (rise, 2, 2),
        (fall, 2, 0),
        (depart, 2, 0),
        (fall, 2, 1),
        (depart, 2, 1),
        (gathered, 3),
        (rise, 3, 0),
        (turn, 1),
        (rise, 3, 1),
        (rise, 3, 2),
        (fall, 3, 0),
        (depart, 3, 0),
        (fall, 3, 1),
        (depart, 3, 1),
        (turn, 2),
        (finish, 1),
        (turn, 3),
        (depart, 0, 0),
        (depart, 0, 1),
        (finish, 2),
        (finish, 3),
        (turn, 0),
        (cross, 2),
        (finish, 0),
    )
    for stage, *at in plan:
        stage(*at)
    total = own_ref[...].astype(jnp.float32) + column[0].astype(jnp.float32)
    def landed(h, z):
        if h is None:
            sender(column.at[0], last_in.at[z], rz[0].at[0, 0], rz[1].at[0, z], near).wait_recv()
        else:
            part = last_in.at[z, :, halves[h]]
            sender(part, part, rz[0].at[h, 0], rz[1].at[h, z], near).wait_recv()

    landed(None, z_near)
    total = total + last_in[z_near].astype(jnp.float32)

    @pl.when(outer)
    def _():
        landed(None, across[2])
        landed(None, z_far)

    @pl.when(middle)
    def _():
        landed(0, z_far)
        landed(1, z_far)
        last_in[me_z] = jnp.zeros(last_in.shape[1:], last_in.dtype)

    total = total + last_in[z_far].astype(jnp.float32)
    last = jnp.where(middle, me_z, across[2])
    total = total + last_in[pl.ds(last, 1)][0].astype(jnp.float32)
    out_ref[...] = total.astype(jnp.bfloat16)
    for copies in pair:
        for copy in copies:
            copy.wait_send()
    for copy in square_copies + w_swaps:
        copy.wait_send()

    @pl.when(outer)
    def _():
        for copy in list(inward.values()) + homeward:
            copy.wait_send()

    @pl.when(middle)
    def _():
        for copy in list(crossing.values()) + list(outward.values()) + mid_sent + crossed:
            copy.wait_send()

    for copy in sent:
        copy.wait_send()


def dense_local(
    lru_input,
    gate_input,
    documents,
    conv_taps,
    rate_weight,
    inlet_weight,
    decay_param,
    lru_gain,
    out_weight,
    residual,
    ffn_gain,
    routes,
    route_weights,
    w_gate,
    w_up,
    w_down,
):
    n_sp, n_tp = lax.axis_size("sp"), lax.axis_size("tp")
    n_z = n_tp // 2
    rows, channels = lru_input.shape
    width = residual.shape[1]
    ff = w_gate.shape[2]
    piece = rows // n_tp
    padded = -(-n_sp // 8) * 8
    vmem = pl.BlockSpec(memory_space=pltpu.VMEM)
    half = width // 2
    top = routes.shape[1]
    hbm = pl.BlockSpec(memory_space=pltpu.HBM)
    bf16, f32 = jnp.bfloat16, jnp.float32
    dma = pltpu.SemaphoreType.DMA
    rows_buffer = pltpu.VMEM((n_z, piece, width), bf16)
    half_buffer = pltpu.VMEM((n_z, piece, half), bf16)
    groups = pltpu.VMEM((n_z, n_sp, piece, width), bf16)
    square_buffer = pltpu.VMEM((n_z, 8, LANES), f32)
    shapes = (
        [(n_sp,)] * 8
        + [(2, n_z)] * 2
        + [(2, n_z + 2)] * 2
        + [(n_z,)] * 2
        + [(2, n_z + 2)] * 2
        + [(4, n_z)] * 2
        + [(2, n_z)] * 2
        + [(3,)] * 2
        + [(4, n_z)] * 2
        + [(2, n_z)] * 2
        + [(2, n_z)] * 2
    )
    return pl.pallas_call(
        functools.partial(layer_kernel, n_sp, n_tp),
        out_shape=pltpu.VMEM((piece, width), bf16),
        in_specs=[hbm] * 16,
        out_specs=vmem,
        scratch_shapes=[
            pltpu.VMEM((rows, channels), bf16),
            pltpu.VMEM((rows, channels), bf16),
            pltpu.VMEM((1, rows), jnp.int32),
            pltpu.VMEM(conv_taps.shape, bf16),
            pltpu.VMEM(rate_weight.shape, bf16),
            pltpu.VMEM(inlet_weight.shape, bf16),
            pltpu.VMEM((1, channels), f32),
            pltpu.VMEM((1, channels), f32),
            pltpu.VMEM((channels, width), bf16),
            pltpu.VMEM((1, width), f32),
            pltpu.VMEM((top, rows), jnp.int32),
            pltpu.VMEM((top, rows), f32),
            pltpu.VMEM((rows, LANES), jnp.int32),
            pltpu.VMEM((padded, rows), f32),
            pltpu.VMEM((32, channels), bf16),
            pltpu.VMEM((n_sp, 32, channels), bf16),
            pltpu.VMEM((8, LANES), jnp.int32),
            pltpu.VMEM((n_sp, 8, LANES), jnp.int32),
            pltpu.VMEM((8, channels), f32),
            pltpu.VMEM((n_sp, 8, channels), f32),
            pltpu.VMEM((n_sp, 8, channels), f32),
            pltpu.VMEM((n_sp, 8, channels), f32),
            pltpu.VMEM((n_sp, padded, rows), f32),
            pltpu.VMEM((rows, channels), f32),
            pltpu.VMEM((rows, channels), f32),
            pltpu.VMEM((n_tp, piece, width), bf16),
            rows_buffer,
            rows_buffer,
            rows_buffer,
            rows_buffer,
            rows_buffer,
            pltpu.VMEM((n_tp, 8, LANES), f32),
            square_buffer,
            square_buffer,
            square_buffer,
            pltpu.VMEM((piece, width), bf16),
            pltpu.VMEM((piece, width), bf16),
            pltpu.VMEM((piece, width), bf16),
            pltpu.VMEM((2, width, ff), bf16),
            pltpu.VMEM((2, width, ff), bf16),
            pltpu.VMEM((2, ff, width), bf16),
            pltpu.VMEM((n_sp, rows, LANES), f32),
            groups,
            pltpu.VMEM((n_sp * piece, 2 * ff), bf16),
            groups,
            pltpu.VMEM((2, n_z, piece, half), bf16),
            pltpu.VMEM((2, n_z, piece, half), bf16),
            half_buffer,
            half_buffer,
            half_buffer,
            half_buffer,
            pltpu.VMEM((piece, width), bf16),
            rows_buffer,
            rows_buffer,
            dma((12,)),
            dma,
            dma((3,)),
            dma,
        ]
        + [dma(shape) for shape in shapes],
        compiler_params=pltpu.CompilerParams(
            collective_id=0, has_side_effects=True, vmem_limit_bytes=48 * 2**20
        ),
    )(
        *(pltpu.with_memory_space_constraint(operand, pltpu.HBM) for operand in (
        lru_input,
        gate_input,
        documents[None, :],
        conv_taps,
        rate_weight,
        inlet_weight,
        decay_param[None, :],
        lru_gain[None, :],
        out_weight,
        residual,
        ffn_gain[None, :],
        routes.T,
        route_weights.T,
        w_gate[0],
        w_up[0],
        w_down[0],
        ))
    )


def solution(mesh):
    n_sp, n_tp = mesh.shape["sp"], mesh.shape["tp"]
    body = dense_local if n_sp == 4 and n_tp == 8 else local
    return jax.shard_map(
        body,
        mesh=mesh,
        in_specs=(
            P("sp", "tp"),
            P("sp", "tp"),
            P("sp"),
            P(None, "tp"),
            P("tp", None, None),
            P("tp", None, None),
            P("tp"),
            P("tp"),
            P("tp", None),
            P("sp", None),
            P(),
            P("sp", None),
            P("sp", None),
            P("sp", None, "tp"),
            P("sp", None, "tp"),
            P("sp", "tp", None),
        ),
        out_specs=P(("sp", "tp"), None),
        check_vma=False,
    )
```
